256 devices in a mesh: sp: 32 (over z, x), tp: 8 (over y, core).
Axes of the slice: x: 4, y: 4, z: 8, core: 2. Of those that a mesh axis runs over, the one named last changes fastest.
Arguments:
- mixer_input: bfloat16 [8192, 1024], P('sp', 'tp'), may hold values from -8 to 8
- decay_shift: float32 [8192, 64], P('sp', 'tp'), may hold values from -2.3 to 0
- pole_real: float32 [64, 64], P('tp'), may hold values from -1 to 0
- pole_imaginary: float32 [64, 64], P('tp'), may hold values from 1 to 201.06176
- log_step: float32 [64], P('tp'), may hold values from -4.15 to -3
- input_map: float32 [2, 64, 64, 16], P(None, 'tp'), may hold values from -1 to 1
- readout_matrix: float32 [2, 64, 16, 64], P(None, 'tp'), may hold values from -0.5 to 0.5
- skip: float32 [1024], P('tp'), may hold values from -6 to 6
- out_proj: bfloat16 [1024, 2048], P('tp'), may hold values from -0.1875 to 0.1875
- stream: bfloat16 [8192, 2048], P(('sp', 'tp')), may hold values from -6 to 6
- norm_gain: float32 [2048], replicated, may hold values from 0.1 to 1.9
- routes: int32 [8192, 2], P(('sp', 'tp')), may hold values from 0 to 31, all different within a row; in each aligned block of 32 rows (0 to 31, 32 to 63, ...) at most 4 rows name the same one
- route_logits: float32 [8192, 2], P(('sp', 'tp')), may hold values from -7.5 to 7.5
- w_gate: bfloat16 [32, 2048, 7168], P('sp', None, 'tp'), may hold values from -0.125 to 0.125
- w_up: bfloat16 [32, 2048, 7168], P('sp', None, 'tp'), may hold values from -0.125 to 0.125
- w_down: bfloat16 [32, 7168, 2048], P('sp', 'tp'), may hold values from -0.21875 to 0.21875
Outputs:
- layer_out: bfloat16 [8192, 2048], P(('sp', 'tp'))
The draws below stay inside these ranges and needn't reach their ends.
Inputs may be any that keep to these rules, and one draw needn't show every extreme that they name: `routes`: in the rows of one device no expert is named more than 4 times, a bound that some block reaches; the 2 experts of a token differ.
All inputs are finite; a program needn't handle non-finite values.
Results may differ from the reference program's by a relative error of at most 0.015.
Values may be sent and summed in bfloat16 or wider, within the bound.
No kernel may reach another device: no remote copies, remote signals or barrier semaphores. Data moves between devices by JAX's collectives and lax.ppermute only.
A program may use at most 64 MiB of HBM per device.

```python
import math
import jax
import jax.numpy as jnp
import numpy as np
from jax import lax

D = 2048
GROUPS = 64
GROUP_CH = 16
STATE = 64
EXPERT_FF = 7168
TOP = 2
SEQUENCE_LOCAL = 256
MIXER_CHANNELS = 1024
SEQ = 8192
TOK_DEV = 32
EXPERTS = 32
CAP = 4
N_TP = 8


def quick_groups(key, count):
    order = jax.random.permutation(jax.random.fold_in(key, 101), GROUPS)
    return order < count


def step_logs(key, quick):
    keys = jax.random.split(jax.random.fold_in(key, 211), 2)
    fast = jax.random.uniform(keys[0], (GROUPS,), jnp.float32, -4.15, -3.88)
    slow = jax.random.uniform(keys[1], (GROUPS,), jnp.float32, -3.9, -3.0)
    return jnp.where(quick, fast, slow)


def draw_log_step(key, part):
    count = GROUPS // 2
    return step_logs(key, quick_groups(key, count))


def draw_pole_real(key, part):
    count = GROUPS // 2
    quick = quick_groups(key, count)
    keys = jax.random.split(jax.random.fold_in(key, 11), 2)
    quick_rate = jax.random.uniform(keys[0], (GROUPS, STATE), jnp.float32, 0.6, 1.0)
    slow_rate = jnp.exp(jax.random.uniform(keys[1], (GROUPS, STATE), jnp.float32, math.log(2.0 / SEQ), math.log(20.0 / SEQ)))
    return -jnp.where(quick[:, None], quick_rate, slow_rate)


def draw_pole_imaginary(key, part):
    count = GROUPS // 2
    quick = quick_groups(key, count)
    step = jnp.exp(step_logs(key, quick))
    keys = jax.random.split(jax.random.fold_in(key, 307), 3)
    spread_poles = jax.random.uniform(keys[0], (GROUPS, STATE), jnp.float32, 1.0, 3.14159 * STATE)
    jitter = jax.random.uniform(keys[1], (GROUPS, STATE), jnp.float32, -0.03, 0.03)
    adjusted = jnp.minimum((3.14159 + jitter) / step[:, None], 3.14159 * STATE)
    chosen = jax.random.randint(keys[2], (GROUPS, STATE), 0, 3) == 0
    return jnp.where(quick[:, None] & chosen, adjusted, spread_poles)


def draw_decay_shift(key, part):
    count = GROUPS // 2
    quick = quick_groups(key, count)
    keys = jax.random.split(jax.random.fold_in(key, 23), 5)
    blocks = SEQ // SEQUENCE_LOCAL
    level = jnp.exp(jax.random.uniform(keys[0], (blocks, GROUPS), jnp.float32, math.log(0.25), math.log(2.0)))
    pieces = jnp.exp(jax.random.uniform(keys[1], (SEQ // 32, GROUPS), jnp.float32, math.log(0.5), math.log(2.0)))
    rough = jax.random.uniform(keys[2], (SEQ, GROUPS), jnp.float32, 0.5, 1.5)
    rate = jnp.where(quick, 0.015, 0.8 / SEQ)
    steady = -jnp.repeat(level, SEQUENCE_LOCAL, axis=0) * jnp.repeat(pieces, 32, axis=0) * rough * rate[None, :]
    spots = jax.random.randint(keys[3], (3,), 0, SEQ)
    losses = jax.random.uniform(keys[4], (3, GROUPS), jnp.float32, math.log(0.5), math.log(0.8))
    hits = (jnp.arange(SEQ, dtype=jnp.int32)[:, None] == spots[None, :]).astype(jnp.float32)
    return steady + jnp.dot(hits, losses, precision=lax.Precision.HIGHEST)


def draw_mixer_input(key, part):
    keys = jax.random.split(jax.random.fold_in(key, 401), 2)
    noise = jnp.clip(jax.random.normal(keys[0], (SEQ, MIXER_CHANNELS), jnp.float32), -6.0, 6.0)
    amplitude = jax.random.uniform(keys[1], (MIXER_CHANNELS,), jnp.float32, -2.0, 2.0)
    parity = (1 - 2 * (jnp.arange(SEQ, dtype=jnp.int32) % 2)).astype(jnp.float32)
    return (noise + parity[:, None] * amplitude[None, :]).astype(jnp.bfloat16)


def draw_route_logits(key, part):
    keys = jax.random.split(jax.random.fold_in(key, 503), 3)
    leading = jnp.clip(1.5 * jax.random.normal(keys[0], (SEQ,), jnp.float32), -4.5, 4.5)
    spacing = jax.random.uniform(keys[1], (SEQ,), jnp.float32, 2.0, 3.0)
    direction = (2 * jax.random.randint(keys[2], (SEQ,), 0, 2) - 1).astype(jnp.float32)
    return jnp.stack([leading, leading - direction * spacing], axis=1)


def levels(key, dims, cuts, least, top_value):
    factor_of, own = 1.0, jax.random.fold_in(key, 6)
    for axis_at, parts in cuts:
        heights = jnp.exp(jax.random.uniform(jax.random.fold_in(own, axis_at), (parts,), jnp.float32, least / len(cuts), top_value / len(cuts)))
        factor_of = factor_of * jnp.repeat(heights, dims[axis_at] // parts).reshape([-1 if axis == axis_at else 1 for axis in range(len(dims))])
    return factor_of


def assign_block(rng, own, number, rows, amount, top, most, lean):
    sequence = jax.random.permutation(rng, amount)
    crowded, common = shares(amount, rows * top, most, lean, True), shares(amount, rows * top, most, lean, False)
    places = jnp.arange(amount)

    def named(sizes, offset_by):
        used = int((sizes > 0).sum())
        fixed = max(1, used // 4)
        moved = fixed + (places - fixed + offset_by * (used - fixed)) % max(1, amount - fixed)
        return jnp.zeros((amount,), jnp.int32).at[sequence[jnp.where(places < fixed, places, moved)]].set(jnp.asarray(sizes, jnp.int32))

    sizes = jnp.where(number % 4 == 0, named(crowded, number // 4), named(common, number - number // 4 - 1))
    mixed = jax.random.permutation(jax.random.fold_in(own, 3), amount)
    source_of, receiver = mixed[0:amount // 2 * 2:2], mixed[1:amount // 2 * 2:2]
    slack = jnp.minimum(sizes[source_of] - 1, most - sizes[receiver]) // 2
    slack = jnp.where((source_of == sequence[0]) | (receiver == sequence[0]) | (sizes[receiver] == 0), 0, jnp.maximum(slack, 0))
    moved = jax.random.randint(jax.random.fold_in(own, 4), (amount // 2,), 0, 1 << 20) % (slack + 1)
    sizes = sizes.at[source_of].add(-moved).at[receiver].add(moved)
    items = jnp.searchsorted(jnp.cumsum(sizes), jnp.arange(rows * top), side="right").astype(jnp.int32)
    table = items.reshape(top, rows).T
    table = table[jax.random.permutation(jax.random.fold_in(own, 1), rows)]
    offset_by = jax.random.randint(jax.random.fold_in(own, 2), (rows, 1), 0, top)
    return jnp.take_along_axis(table, (jnp.arange(top)[None, :] + offset_by) % top, axis=1)


def shares(number_of, total, reach, slope, full):
    weights = [(1 << 20) // math.isqrt(rank ** slope) + 1 for rank in range(1, number_of + 1)]
    largest = reach if full else min(reach, max(-(-total // number_of), total * weights[0] // sum(weights)))
    least = 1 if total - largest >= number_of - 1 else 0
    counts, rest = [largest] + [least] * (number_of - 1), total - largest - least * (number_of - 1)
    while rest > 0:
        free = [i for i in range(1, number_of) if counts[i] < largest] or [i for i in range(1, number_of) if counts[i] < reach]
        mass, remaining = sum([weights[i] for i in free]), rest
        for i in free:
            addition = min(reach - counts[i], max(1, remaining * weights[i] // mass), rest)
            counts[i] = counts[i] + addition
            rest = rest - addition
    return np.array(counts)


def gaussian(key, extent, spread, most, cuts=(), kind=jnp.bfloat16):
    factor_of = levels(key, extent, cuts, -0.22, 0.18) if cuts else 1.0
    entries = jax.random.normal(key, extent, jnp.float32) * spread * factor_of
    return jnp.minimum(jnp.maximum(entries, -most), most).astype(kind)


def setup_inputs(seed: int = 0) -> dict:
    key_list = jax.random.split(jax.random.key(seed), 17)
    mixer_input = draw_mixer_input(jax.random.fold_in(key_list[16], 71), 0)
    decay_shift = draw_decay_shift(jax.random.fold_in(key_list[16], 71), 0)
    pole_real = draw_pole_real(jax.random.fold_in(key_list[16], 71), 0)
    pole_imaginary = draw_pole_imaginary(jax.random.fold_in(key_list[16], 71), 0)
    log_step = draw_log_step(jax.random.fold_in(key_list[16], 71), 0)
    input_map = gaussian(key_list[5], (2, GROUPS, STATE, GROUP_CH), (2 * GROUP_CH) ** -0.5, 1.0, ((1, 8),), jnp.float32)
    readout_matrix = gaussian(key_list[6], (2, GROUPS, GROUP_CH, STATE), (2 * STATE) ** -0.5, 0.5, ((1, 8),), jnp.float32)
    skip = gaussian(key_list[7], (MIXER_CHANNELS,), 1.0, 6.0, ((0, 8),), jnp.float32)
    out_proj = gaussian(key_list[8], (MIXER_CHANNELS, D), MIXER_CHANNELS ** -0.5, 0.1875, ((0, 8),))
    stream = gaussian(key_list[9], (SEQ, D), 1.0, 6.0, ((0, 256),))
    norm_gain = jnp.clip(1.0 + 0.18 * jax.random.normal(key_list[10], (D,), jnp.float32), 0.1, 1.9)
    routes_keys = jax.random.split(jax.random.fold_in(key_list[11], 1), SEQ // TOK_DEV)
    routes_turns = jax.random.permutation(jax.random.fold_in(key_list[11], 3), SEQ // TOK_DEV)
    routes = jax.vmap(lambda own, number: assign_block(jax.random.fold_in(key_list[11], 2), own, number, TOK_DEV, EXPERTS, TOP, CAP, 2))(routes_keys, routes_turns).reshape((SEQ, TOP))
    route_logits = draw_route_logits(jax.random.fold_in(key_list[16], 71), 0)
    w_gate = gaussian(key_list[13], (EXPERTS, D, EXPERT_FF), D ** -0.5, 0.125, ((0, 32), (2, 8)))
    w_up = gaussian(key_list[14], (EXPERTS, D, EXPERT_FF), D ** -0.5, 0.125, ((0, 32), (2, 8)))
    w_down = gaussian(key_list[15], (EXPERTS, EXPERT_FF, D), (EXPERT_FF // 9) ** -0.5, 0.21875, ((0, 32), (1, 8)))
    return dict(mixer_input=mixer_input, decay_shift=decay_shift, pole_real=pole_real, pole_imaginary=pole_imaginary, log_step=log_step, input_map=input_map, readout_matrix=readout_matrix, skip=skip, out_proj=out_proj, stream=stream, norm_gain=norm_gain, routes=routes, route_logits=route_logits, w_gate=w_gate, w_up=w_up, w_down=w_down)


TOP_PRECISION = lax.Precision.HIGHEST
EPS = 1e-06
SEGMENT = 16

def discretize(pole_real, pole_imaginary, log_step, input_map):
    step = jnp.exp(log_step)[:, None]
    magnitude = jnp.exp(pole_real * step)
    factor_real = magnitude * jnp.cos(pole_imaginary * step)
    factor_imaginary = magnitude * jnp.sin(pole_imaginary * step)
    denominator = pole_real * pole_real + pole_imaginary * pole_imaginary
    ratio_real = ((factor_real - 1.0) * pole_real + factor_imaginary * pole_imaginary) / denominator
    ratio_imaginary = (factor_imaginary * pole_real - (factor_real - 1.0) * pole_imaginary) / denominator
    map_real = ratio_real[:, :, None] * input_map[0] - ratio_imaginary[:, :, None] * input_map[1]
    map_imaginary = ratio_real[:, :, None] * input_map[1] + ratio_imaginary[:, :, None] * input_map[0]
    return (factor_real, factor_imaginary, map_real, map_imaginary)

def link(earlier, later):
    a_real, a_imag_part, x_real, x_imag_part = earlier
    b_real, b_imag_part, y_real, y_imag_part = later
    return (b_real * a_real - b_imag_part * a_imag_part, b_real * a_imag_part + b_imag_part * a_real, b_real * x_real - b_imag_part * x_imag_part + y_real, b_real * x_imag_part + b_imag_part * x_real + y_imag_part)

def block_states(drive_input, shift, factors):
    factor_real, factor_imaginary, map_real, map_imaginary = factors
    rows, groups = shift.shape
    states = factor_real.shape[1]
    width = groups * states
    grouped = drive_input.reshape(rows, groups, -1)
    drive_real = jnp.einsum('sgc,gpc->sgp', grouped, map_real, precision=TOP_PRECISION).reshape(rows, width)
    drive_imaginary = jnp.einsum('sgc,gpc->sgp', grouped, map_imaginary, precision=TOP_PRECISION).reshape(rows, width)
    scale = jnp.exp(shift)[:, :, None]
    trans_real = (scale * factor_real[None]).reshape(rows, width)
    trans_imaginary = (scale * factor_imaginary[None]).reshape(rows, width)
    segments = rows // SEGMENT

    def arrange(value):
        return jnp.swapaxes(value.reshape(segments, SEGMENT, width), 0, 1)

    def advance(carry, item):
        new = link(carry, item)
        return (new, new)
    first = jnp.ones((segments, width), jnp.float32)
    empty = jnp.zeros((segments, width), jnp.float32)
    _, inner = lax.scan(advance, (first, empty, empty, empty), (arrange(trans_real), arrange(trans_imaginary), arrange(drive_real), arrange(drive_imaginary)))
    totals = tuple((part[-1] for part in inner))
    running = lax.associative_scan(link, totals, axis=0)
    enter = tuple((jnp.concatenate([start, part[:-1]], axis=0) for start, part in zip((first[:1], empty[:1], empty[:1], empty[:1]), running)))
    enter = tuple((part.reshape(segments, width) for part in enter))
    joined = link(tuple((part[None] for part in enter)), inner)

    def restore(value):
        return jnp.swapaxes(value, 0, 1).reshape(rows, groups, states)
    return tuple((restore(part) for part in joined))

def read_out(hidden_state_real, hidden_state_imaginary, readout_matrix):
    return jnp.einsum('ani,nyi->any', hidden_state_real, readout_matrix[0], precision=TOP_PRECISION) - jnp.einsum('ani,nyi->any', hidden_state_imaginary, readout_matrix[1], precision=TOP_PRECISION)

def reference(mixer_input, decay_shift, pole_real, pole_imaginary, log_step, input_map, readout_matrix, skip, out_proj, stream, norm_gain, routes, route_logits, w_gate, w_up, w_down):
    factors = discretize(pole_real, pole_imaginary, log_step, input_map)
    blocks = SEQ // SEQUENCE_LOCAL
    inputs_blocked = mixer_input.astype(jnp.float32).reshape(blocks, SEQUENCE_LOCAL, MIXER_CHANNELS)
    shift_blocked = decay_shift.reshape(blocks, SEQUENCE_LOCAL, GROUPS)

    def advance(carry, pair):
        drive_input, shift = pair
        through_real, through_imaginary, local_real, local_imaginary = block_states(drive_input, shift, factors)
        enter_real, enter_imaginary = carry
        hidden_state_real = local_real + through_real * enter_real[None] - through_imaginary * enter_imaginary[None]
        hidden_state_imaginary = local_imaginary + through_real * enter_imaginary[None] + through_imaginary * enter_real[None]
        response = read_out(hidden_state_real, hidden_state_imaginary, readout_matrix).reshape(SEQUENCE_LOCAL, MIXER_CHANNELS) + skip * drive_input
        activated = jax.nn.gelu(response).astype(jnp.bfloat16)
        return ((hidden_state_real[-1], hidden_state_imaginary[-1]), activated)
    start = (jnp.zeros((GROUPS, STATE), jnp.float32), jnp.zeros((GROUPS, STATE), jnp.float32))
    _, activated = lax.scan(advance, start, (inputs_blocked, shift_blocked))
    projected = jnp.dot(activated.reshape(SEQ, MIXER_CHANNELS), out_proj, preferred_element_type=jnp.float32)
    mixed = (stream.astype(jnp.float32) + projected).astype(jnp.bfloat16)
    mixed_wide = mixed.astype(jnp.float32)
    normed = (mixed_wide * lax.rsqrt(lax.optimization_barrier(jnp.mean(mixed_wide * mixed_wide, axis=-1, keepdims=True)) + EPS) * norm_gain).astype(jnp.bfloat16)
    device_blocks = SEQ // TOK_DEV
    assign = routes.reshape(device_blocks, TOK_DEV * TOP)
    matches = (assign[:, :, None] == jnp.arange(EXPERTS, dtype=jnp.int32)).astype(jnp.int32)
    rank = lax.optimization_barrier(jnp.sum((jnp.cumsum(matches, axis=1) - matches) * matches, axis=2))
    block_ids = jnp.broadcast_to(jnp.arange(device_blocks, dtype=jnp.int32)[:, None], assign.shape)
    token_ids = (jnp.arange(SEQ * TOP, dtype=jnp.int32) // TOP).reshape(device_blocks, TOK_DEV * TOP)
    buffer = jnp.zeros((EXPERTS, device_blocks, CAP, D), jnp.bfloat16)
    buffer = buffer.at[assign, block_ids, rank].set(normed[token_ids])

    def run_expert(pack):
        rows, gate_weight, upward_weight, down_weight = pack
        flat = rows.reshape(device_blocks * CAP, D)
        gate = jnp.dot(flat, gate_weight, preferred_element_type=jnp.float32)
        upward = jnp.dot(flat, upward_weight, preferred_element_type=jnp.float32)
        hidden = (jax.nn.silu(gate) * upward).astype(jnp.bfloat16)
        width = EXPERT_FF // N_TP
        summed = jnp.zeros((device_blocks * CAP, D), jnp.float32)
        for part_index in range(N_TP):
            partial_out = jnp.dot(hidden[:, part_index * width:(part_index + 1) * width], down_weight[part_index * width:(part_index + 1) * width], preferred_element_type=jnp.float32)
            summed = summed + lax.optimization_barrier(partial_out.astype(jnp.bfloat16)).astype(jnp.float32)
        return summed.astype(jnp.bfloat16).reshape(device_blocks, CAP, D)
    outputs = lax.map(run_expert, (buffer, w_gate, w_up, w_down))
    picked = outputs[assign, block_ids, rank].astype(jnp.float32).reshape(SEQ, TOP, D)
    logits = route_logits
    weights = jax.nn.sigmoid(jnp.stack([logits[:, 0] - logits[:, 1], logits[:, 1] - logits[:, 0]], axis=1))
    combined = mixed_wide + lax.optimization_barrier(jnp.sum(picked * weights[:, :, None], axis=1))
    return combined.astype(jnp.bfloat16)
```

```python
import jax
import jax.numpy as jnp
from jax import lax
from jax.sharding import PartitionSpec as P

TOP_PRECISION = lax.Precision.HIGHEST
EPS = 1e-06
SEGMENT = 16


def from_everyone(array, axis):
    size = lax.axis_size(axis)
    return lax.all_to_all(
        jnp.broadcast_to(array[None], (size, *array.shape)), axis, 0, 0, tiled=True
    )


def all_in_one(array, axis):
    leaves = jax.tree.leaves(array)
    sequence = sorted(range(len(leaves)), key=lambda k: -leaves[k].size)
    width = (1, *leaves[sequence[0]].shape)[-1]
    lines = [
        jnp.pad(leaves[k].reshape(-1), (0, -leaves[k].size % width)).reshape(-1, width)
        for k in sequence
    ]
    both, at, found = (from_everyone(jnp.concatenate(lines), axis), 0, {})
    for k, line in zip(sequence, lines):
        slab = both[:, at : at + len(line)].reshape(len(both), -1)
        found[k] = slab[:, : leaves[k].size].reshape(-1, *leaves[k].shape)
        at += len(line)
    numbers = iter(range(len(leaves)))
    return jax.tree.map(lambda _: found[next(numbers)], array)


def combined_pairwise(pieces, combine):
    while len(jax.tree.leaves(pieces)[0]) > 1:
        pieces = jax.vmap(combine)(
            *(jax.tree.map(lambda part: part[side::2], pieces) for side in (0, 1))
        )
    return jax.tree.map(lambda part: part[0], pieces)


def entering(array, axis, combine, identity):
    size, here = (lax.axis_size(axis), lax.axis_index(axis))
    passed = jnp.arange(size) < here

    def kept(part, zero, own):
        part = jnp.where(
            passed.reshape(-1, *(1 for _ in own.shape)), part, jnp.asarray(zero, own.dtype)
        )
        return part

    pieces = all_in_one(array, axis)
    return combined_pairwise(jax.tree.map(kept, pieces, identity, array), combine)


def cut_along(array, dim, size):
    shape = array.shape
    blocks = array.reshape(*shape[:dim], size, shape[dim] // size, *shape[dim + 1 :])
    return jnp.moveaxis(blocks, dim, 0)


def sum_at_owner(array, axis, dim):
    blocks = cut_along(array, dim, lax.axis_size(axis))
    arrived = lax.all_to_all(blocks, axis, split_axis=0, concat_axis=0, tiled=True)
    return arrived.astype(jnp.float32).sum(axis=0)


def discretize(pole_real, pole_imaginary, log_step, input_map):
    step = jnp.exp(log_step)[:, None]
    magnitude = jnp.exp(pole_real * step)
    factor_real = magnitude * jnp.cos(pole_imaginary * step)
    factor_imaginary = magnitude * jnp.sin(pole_imaginary * step)
    denominator = pole_real * pole_real + pole_imaginary * pole_imaginary
    ratio_real = ((factor_real - 1.0) * pole_real + factor_imaginary * pole_imaginary) / denominator
    ratio_imaginary = (
        factor_imaginary * pole_real - (factor_real - 1.0) * pole_imaginary
    ) / denominator
    map_real = ratio_real[:, :, None] * input_map[0] - ratio_imaginary[:, :, None] * input_map[1]
    map_imaginary = (
        ratio_real[:, :, None] * input_map[1] + ratio_imaginary[:, :, None] * input_map[0]
    )
    return (factor_real, factor_imaginary, map_real, map_imaginary)


def link(earlier, later):
    a_real, a_imag_part, x_real, x_imag_part = earlier
    b_real, b_imag_part, y_real, y_imag_part = later
    return (
        b_real * a_real - b_imag_part * a_imag_part,
        b_real * a_imag_part + b_imag_part * a_real,
        b_real * x_real - b_imag_part * x_imag_part + y_real,
        b_real * x_imag_part + b_imag_part * x_real + y_imag_part,
    )


def block_states(drive_input, shift, factors):
    factor_real, factor_imaginary, map_real, map_imaginary = factors
    rows, groups = shift.shape
    states = factor_real.shape[1]
    width = groups * states
    grouped = drive_input.reshape(rows, groups, -1)
    drive_real = jnp.einsum("sgc,gpc->sgp", grouped, map_real, precision=TOP_PRECISION).reshape(
        rows, width
    )
    drive_imaginary = jnp.einsum(
        "sgc,gpc->sgp", grouped, map_imaginary, precision=TOP_PRECISION
    ).reshape(rows, width)
    scale = jnp.exp(shift)[:, :, None]
    trans_real = (scale * factor_real[None]).reshape(rows, width)
    trans_imaginary = (scale * factor_imaginary[None]).reshape(rows, width)
    segments = rows // SEGMENT

    def arrange(value):
        return jnp.swapaxes(value.reshape(segments, SEGMENT, width), 0, 1)

    def advance(carry, item):
        new = link(carry, item)
        return (new, new)

    first = jnp.ones((segments, width), jnp.float32)
    empty = jnp.zeros((segments, width), jnp.float32)
    _, inner = lax.scan(
        advance,
        (first, empty, empty, empty),
        (
            arrange(trans_real),
            arrange(trans_imaginary),
            arrange(drive_real),
            arrange(drive_imaginary),
        ),
    )
    totals = tuple((part[-1] for part in inner))
    running = lax.associative_scan(link, totals, axis=0)
    enter = tuple(
        (
            jnp.concatenate([start, part[:-1]], axis=0)
            for start, part in zip((first[:1], empty[:1], empty[:1], empty[:1]), running)
        )
    )
    enter = tuple((part for part in enter))
    joined = link(tuple((part[None] for part in enter)), inner)

    def restore(value):
        return jnp.swapaxes(value, 0, 1).reshape(rows, groups, states)

    return tuple((restore(part) for part in joined))


def read_out(hidden_state_real, hidden_state_imaginary, readout_matrix):
    return jnp.einsum(
        "ani,nyi->any", hidden_state_real, readout_matrix[0], precision=TOP_PRECISION
    ) - jnp.einsum(
        "ani,nyi->any", hidden_state_imaginary, readout_matrix[1], precision=TOP_PRECISION
    )


def slot_numbers(route_rows, experts, capacity):
    flat = route_rows.reshape(route_rows.shape[:-2] + (-1,))
    matches = (flat[..., None] == jnp.arange(experts, dtype=jnp.int32)).astype(jnp.int32)
    earlier = jnp.cumsum(matches, axis=-2) - matches
    return flat * capacity + jnp.sum(earlier * matches, axis=-1)


def dispatch_rows(slots, normed, width):
    hits = (slots[..., None] == jnp.arange(width, dtype=jnp.int32)).astype(jnp.bfloat16)
    tokens = normed.shape[-2]
    hits = hits.reshape(slots.shape[:-1] + (tokens, -1, width)).sum(axis=-2)
    return jnp.einsum(
        "...tw,...td->...wd", hits, normed, preferred_element_type=jnp.float32
    ).astype(jnp.bfloat16)


def chip_shift(distance, flip=0):
    size = lax.axis_size("tp")
    chips = size // 2
    return [
        (2 * chip + core, 2 * ((chip + distance) % chips) + (core ^ flip))
        for chip in range(chips)
        for core in range(2)
    ]


def gathered_projection(out_proj, ready):
    out_proj, _ = lax.optimization_barrier((out_proj, ready))
    chips = lax.axis_size("tp") // 2
    blocks = [out_proj] + [
        lax.ppermute(out_proj, "tp", chip_shift(distance)) for distance in range(1, chips)
    ]
    mine = jnp.concatenate(blocks, axis=0)
    other = lax.ppermute(mine, "tp", chip_shift(0, 1))
    return mine, other


def project_own(activated, wide_proj, own_rows):
    size = lax.axis_size("tp")
    chips = size // 2
    here = lax.axis_index("tp")
    chip, core = here // 2, here % 2
    arrived = lax.all_to_all(
        activated.reshape(size, own_rows, -1), "tp", split_axis=0, concat_axis=0, tiled=True
    )

    def parity_rows(parity):
        return jnp.concatenate(
            [
                lax.dynamic_index_in_dim(
                    arrived, 2 * ((chip - distance) % chips) + parity, 0, keepdims=False
                )
                for distance in range(chips)
            ],
            axis=1,
        )

    mine, other = wide_proj
    return jnp.dot(
        parity_rows(core), mine, preferred_element_type=jnp.float32
    ) + jnp.dot(parity_rows(1 - core), other, preferred_element_type=jnp.float32)


def expert_over_chips(rows, w_gate, w_up, w_down):
    chips = lax.axis_size("tp") // 2
    held = rows.shape[0]
    rows, w_gate_sent, w_up_sent, w_down_sent = lax.optimization_barrier(
        (rows, w_gate, w_up, w_down)
    )
    fetched = {
        distance: lax.ppermute(rows, "tp", chip_shift(distance)) for distance in (1, 3, 2)
    }
    other = [lax.ppermute(w, "tp", chip_shift(0, 1)) for w in (w_gate_sent, w_up_sent, w_down_sent)]

    def partial_out(block):
        total = None
        for gate_weight, up_weight, down_weight in ((w_gate, w_up, w_down), other):
            gate = jnp.dot(block, gate_weight, preferred_element_type=jnp.float32)
            upward = jnp.dot(block, up_weight, preferred_element_type=jnp.float32)
            hidden = (jax.nn.silu(gate) * upward).astype(jnp.bfloat16)
            part = jnp.dot(hidden, down_weight, preferred_element_type=jnp.float32)
            total = part if total is None else total + part
        return total

    near = partial_out(jnp.concatenate([rows, fetched[1], fetched[3]], axis=0))
    far = partial_out(fetched[2])
    back = [
        lax.ppermute(near[held : 2 * held].astype(jnp.bfloat16), "tp", chip_shift(-1)),
        lax.ppermute(near[2 * held :].astype(jnp.bfloat16), "tp", chip_shift(-3)),
        lax.ppermute(far.astype(jnp.bfloat16), "tp", chip_shift(-2)),
    ]
    total = near[:held]
    for part in back:
        total = total + part.astype(jnp.float32)
    return total.astype(jnp.bfloat16)


def weighted_pick(slots, weights, returned_result):
    width, top = returned_result.shape[0], weights.shape[1]
    hits = slots.reshape(-1, top)[..., None] == jnp.arange(width, dtype=jnp.int32)
    spread = jnp.sum(jnp.where(hits, weights[..., None], 0.0), axis=1)
    high = spread.astype(jnp.bfloat16)
    low = (spread - high.astype(jnp.float32)).astype(jnp.bfloat16)
    return jnp.dot(high, returned_result, preferred_element_type=jnp.float32) + jnp.dot(
        low, returned_result, preferred_element_type=jnp.float32
    )


def shards(
    mixer_input,
    decay_shift,
    pole_real,
    pole_imaginary,
    log_step,
    input_map,
    readout_matrix,
    skip,
    out_proj,
    stream,
    norm_gain,
    routes,
    route_logits,
    w_gate,
    w_up,
    w_down,
):
    factors = discretize(pole_real, pole_imaginary, log_step, input_map)
    drive_input = mixer_input.astype(jnp.float32)
    rows = mixer_input.shape[0]
    groups, states = pole_real.shape
    through_real, through_imaginary, local_real, local_imaginary = block_states(
        drive_input, decay_shift, factors
    )
    ones = jnp.ones((groups, states), jnp.float32)
    zeros = jnp.zeros((groups, states), jnp.float32)
    carried = entering(
        (through_real[-1], through_imaginary[-1], local_real[-1], local_imaginary[-1]),
        "sp",
        link,
        (ones, zeros, zeros, zeros),
    )
    enter_real, enter_imaginary = (carried[2], carried[3])
    extra_real = through_real * enter_real[None] - through_imaginary * enter_imaginary[None]
    extra_imaginary = through_real * enter_imaginary[None] + through_imaginary * enter_real[None]
    response = read_out(local_real + extra_real, local_imaginary + extra_imaginary, readout_matrix)
    response = response.reshape(rows, -1) + skip * drive_input
    activated = jax.nn.gelu(response).astype(jnp.bfloat16)
    own_rows = rows // lax.axis_size("tp")
    model = stream.shape[1]
    wide_proj = gathered_projection(out_proj, carried[2])
    projected = project_own(activated, wide_proj, own_rows)
    mixed = (stream.astype(jnp.float32) + projected).astype(jnp.bfloat16)
    mixed_wide = mixed.astype(jnp.float32)
    normed = (
        mixed_wide
        * lax.rsqrt(jnp.mean(mixed_wide * mixed_wide, axis=-1, keepdims=True) + EPS)
        * norm_gain
    ).astype(jnp.bfloat16)
    weights = jax.nn.sigmoid(
        jnp.stack(
            [route_logits[:, 0] - route_logits[:, 1], route_logits[:, 1] - route_logits[:, 0]],
            axis=1,
        )
    )
    experts = lax.axis_size("sp") * w_gate.shape[0]
    capacity = 4 * own_rows // experts
    slot_width = experts * capacity
    own_slots = slot_numbers(routes, experts, capacity)
    outgoing = dispatch_rows(own_slots, normed, slot_width)
    arrived = lax.all_to_all(
        outgoing.reshape(experts, capacity, model), "sp", split_axis=0, concat_axis=0, tiled=True
    ).reshape(-1, model)
    summed = expert_over_chips(arrived, w_gate[0], w_up[0], w_down[0])
    returned_result = lax.all_to_all(
        summed.reshape(experts, capacity, model), "sp", split_axis=0, concat_axis=0, tiled=True
    ).reshape(slot_width, model)
    combined = mixed_wide + weighted_pick(own_slots, weights, returned_result)
    return combined.astype(jnp.bfloat16)


def solution(mesh):
    return jax.shard_map(
        shards,
        mesh=mesh,
        in_specs=(
            P("sp", "tp"),
            P("sp", "tp"),
            P("tp", None),
            P("tp", None),
            P("tp"),
            P(None, "tp", None, None),
            P(None, "tp", None, None),
            P("tp"),
            P("tp", None),
            P(("sp", "tp"), None),
            P(),
            P(("sp", "tp"), None),
            P(("sp", "tp"), None),
            P("sp", None, "tp"),
            P("sp", None, "tp"),
            P("sp", "tp", None),
        ),
        out_specs=P(("sp", "tp"), None),
        check_vma=False,
    )
```

```python
import functools

import jax
import jax.numpy as jnp
from jax import lax
from jax.experimental import pallas as pl
from jax.experimental.pallas import tpu as pltpu
from jax.sharding import PartitionSpec as P

EPS = 1e-06


LANES = 8
EXACT = lax.Precision.HIGHEST


def one_hot(shape, test):
    rows = lax.broadcasted_iota(jnp.int32, shape, 0)
    columns = lax.broadcasted_iota(jnp.int32, shape, 1)
    return jnp.where(test(rows, columns), 1.0, 0.0).astype(jnp.float32)


def exact_dot(left, right, transposed=False):
    contract = ((1,), (1,)) if transposed else ((1,), (0,))
    return lax.dot_general(
        left, right, (contract, ((), ())), precision=EXACT, preferred_element_type=jnp.float32
    )


def complex_times(a_real, a_imag, b_real, b_imag):
    return a_real * b_real - a_imag * b_imag, a_real * b_imag + a_imag * b_real


def states_kernel(
    input_ref,
    shift_ref,
    pole_real_ref,
    pole_imag_ref,
    log_step_ref,
    map_ref,
    total_ref,
    drive_real_ref,
    drive_imag_ref,
    scale_ref,
    factor_ref,
    enter_ref,
):
    rows = input_ref.shape[0]
    groups, states = pole_real_ref.shape
    width = groups * states
    channels = map_ref.shape[1] // groups
    length = rows // LANES
    spread = one_hot((states, width), lambda r, c: c % states == r)
    group_of = one_hot((groups, width), lambda r, c: c // states == r)

    def in_a_row(ref):
        return jnp.sum(exact_dot(ref[...], spread) * group_of, axis=0, keepdims=True)

    pole_real, pole_imag = in_a_row(pole_real_ref), in_a_row(pole_imag_ref)
    logs = jnp.broadcast_to(log_step_ref[...], (groups, groups))
    step = jnp.exp(exact_dot(logs, group_of)[:1])
    magnitude = jnp.exp(pole_real * step)
    factor_real = magnitude * jnp.cos(pole_imag * step)
    factor_imag = magnitude * jnp.sin(pole_imag * step)
    denominator = pole_real * pole_real + pole_imag * pole_imag
    ratio_real = ((factor_real - 1.0) * pole_real + factor_imag * pole_imag) / denominator
    ratio_imag = (factor_imag * pole_real - (factor_real - 1.0) * pole_imag) / denominator
    factor_ref[0:1, :] = factor_real
    factor_ref[1:2, :] = factor_imag

    order = one_hot((rows, rows), lambda r, c: c == (r % LANES) * length + r // LANES)
    inputs = jnp.dot(
        order.astype(jnp.bfloat16), input_ref[...], preferred_element_type=jnp.float32
    )
    scale_ref[...] = exact_dot(exact_dot(order, jnp.exp(shift_ref[...]), True), group_of)
    same_group = one_hot(
        (groups * channels, width), lambda r, c: r // channels == c // states
    )
    plain_real = exact_dot(inputs, exact_dot(map_ref[0], spread) * same_group)
    plain_imag = exact_dot(inputs, exact_dot(map_ref[1], spread) * same_group)
    drive_real, drive_imag = complex_times(ratio_real, ratio_imag, plain_real, plain_imag)
    drive_real_ref[...] = drive_real
    drive_imag_ref[...] = drive_imag

    wide_real = jnp.broadcast_to(factor_real, (LANES, width))
    wide_imag = jnp.broadcast_to(factor_imag, (LANES, width))
    through_real = jnp.ones((LANES, width), jnp.float32)
    through_imag = state_real = state_imag = jnp.zeros((LANES, width), jnp.float32)
    for k in range(length):
        at = slice(k * LANES, (k + 1) * LANES)
        scale = scale_ref[at, :]
        real, imag = scale * wide_real, scale * wide_imag
        through_real, through_imag = complex_times(real, imag, through_real, through_imag)
        state_real, state_imag = complex_times(real, imag, state_real, state_imag)
        state_real = state_real + drive_real_ref[at, :]
        state_imag = state_imag + drive_imag_ref[at, :]

    place = lax.broadcasted_iota(jnp.int32, (LANES, width), 0)

    def moved(value, by, empty):
        return jnp.where(place >= by, pltpu.roll(value, by, 0), empty)

    by = 1
    while by < LANES:
        a_real, a_imag = moved(through_real, by, 1.0), moved(through_imag, by, 0.0)
        x_real, x_imag = moved(state_real, by, 0.0), moved(state_imag, by, 0.0)
        x_real, x_imag = complex_times(through_real, through_imag, x_real, x_imag)
        state_real, state_imag = state_real + x_real, state_imag + x_imag
        through_real, through_imag = complex_times(through_real, through_imag, a_real, a_imag)
        by *= 2
    enter_ref[0] = moved(through_real, 1, 1.0)
    enter_ref[1] = moved(through_imag, 1, 0.0)
    enter_ref[2] = moved(state_real, 1, 0.0)
    enter_ref[3] = moved(state_imag, 1, 0.0)
    total = jnp.concatenate(
        [v[LANES - 1 :] for v in (through_real, through_imag, state_real, state_imag)], axis=0
    )
    total_ref[...] = jnp.broadcast_to(total[None], total_ref.shape)


def response_kernel(
    here_ref,
    arrived_ref,
    drive_real_ref,
    drive_imag_ref,
    scale_ref,
    factor_ref,
    enter_ref,
    input_ref,
    readout_ref,
    skip_ref,
    out_ref,
    state_ref,
):
    rows = input_ref.shape[0]
    width = factor_ref.shape[1]
    states = readout_ref.shape[2]
    channels = readout_ref.shape[1] * states // width
    length = rows // LANES
    here = here_ref[0]
    carry_real = carry_imag = jnp.zeros((1, width), jnp.float32)
    for j in range(arrived_ref.shape[0]):
        block = arrived_ref[j]
        real, imag = complex_times(block[0:1], block[1:2], carry_real, carry_imag)
        earlier = j < here
        carry_real = jnp.where(earlier, real + block[2:3], carry_real)
        carry_imag = jnp.where(earlier, imag + block[3:4], carry_imag)
    state_real, state_imag = complex_times(enter_ref[0], enter_ref[1], carry_real, carry_imag)
    state_real, state_imag = state_real + enter_ref[2], state_imag + enter_ref[3]
    wide_real = jnp.broadcast_to(factor_ref[0:1, :], (LANES, width))
    wide_imag = jnp.broadcast_to(factor_ref[1:2, :], (LANES, width))
    for k in range(length):
        at = slice(k * LANES, (k + 1) * LANES)
        scale = scale_ref[at, :]
        real, imag = scale * wide_real, scale * wide_imag
        state_real, state_imag = complex_times(real, imag, state_real, state_imag)
        state_real = state_real + drive_real_ref[at, :]
        state_imag = state_imag + drive_imag_ref[at, :]
        state_ref[at, :width] = state_real
        state_ref[at, width:] = state_imag
    spread = one_hot((states, width), lambda r, c: c % states == r)
    same_group = one_hot(
        (readout_ref.shape[1], width), lambda r, c: r // channels == c // states
    )
    matrix = jnp.concatenate(
        [
            exact_dot(readout_ref[0], spread) * same_group,
            exact_dot(readout_ref[1], spread) * -same_group,
        ],
        axis=1,
    )
    response = exact_dot(state_ref[...], matrix, True)
    order = one_hot((rows, rows), lambda r, c: r == (c % LANES) * length + c // LANES)
    response = exact_dot(order, response) + skip_ref[...] * input_ref[...].astype(jnp.float32)
    out_ref[...] = jax.nn.gelu(response).astype(jnp.bfloat16)


def local_states(
    mixer_input, decay_shift, pole_real, pole_imaginary, log_step, input_map, devices
):
    rows = mixer_input.shape[0]
    groups, states = pole_real.shape
    width = groups * states
    f32 = jnp.float32
    shape = jax.ShapeDtypeStruct
    return pl.pallas_call(
        states_kernel,
        out_shape=(
            shape((devices, 4, width), f32),
            shape((rows, width), f32),
            shape((rows, width), f32),
            shape((rows, width), f32),
            shape((2, width), f32),
            shape((4, LANES, width), f32),
        ),
        compiler_params=pltpu.CompilerParams(vmem_limit_bytes=16 << 20),
        name="states",
    )(
        mixer_input,
        decay_shift.T,
        pole_real,
        pole_imaginary,
        log_step[None],
        jnp.swapaxes(input_map, 2, 3).reshape(2, -1, states),
    )


def activations(here, arrived, kept, mixer_input, readout_matrix, skip):
    rows, channels = mixer_input.shape
    width = arrived.shape[2]
    vmem = pl.BlockSpec(memory_space=pltpu.VMEM)
    return pl.pallas_call(
        response_kernel,
        out_shape=jax.ShapeDtypeStruct((rows, channels), jnp.bfloat16),
        in_specs=[pl.BlockSpec(memory_space=pltpu.SMEM)] + [vmem] * 9,
        scratch_shapes=[pltpu.VMEM((rows, 2 * width), jnp.float32)],
        compiler_params=pltpu.CompilerParams(vmem_limit_bytes=16 << 20),
        name="response",
    )(
        here.reshape(1),
        arrived,
        *kept,
        mixer_input,
        readout_matrix.reshape(2, channels, -1),
        skip[None],
    )


def experts_kernel(capacity, first_ref, second_ref, *refs):
    weights, (first_out_ref, second_out_ref), scratch = refs[:6], refs[6:8], refs[8:]
    buffers, semaphores = scratch[:6], scratch[6]
    held = first_ref.shape[0] // 2
    parts = 2

    def copies(index):
        rows = weights[index].shape[0] // parts
        return [
            pltpu.make_async_copy(
                weights[index].at[pl.ds(part * rows, rows)],
                buffers[index].at[pl.ds(part * rows, rows)],
                semaphores.at[index, part],
            )
            for part in range(parts)
        ]

    every = [copies(index) for index in range(6)]
    for base in (0, 3):
        for part in range(parts):
            every[base][part].start()
            every[base + 1][part].start()
        for part in range(parts):
            every[base + 2][part].start()

    def whole_rows(half):
        return one_hot(
            (held, 2 * held),
            lambda r, c: c == r // capacity * (2 * capacity) + r % capacity + half * capacity,
        ).astype(jnp.bfloat16)

    pick = [whole_rows(half) for half in range(2)]
    pieces = [
        jnp.concatenate(
            [
                jnp.dot(pick[half], ref[...], preferred_element_type=jnp.float32)
                for ref in (first_ref, second_ref)
            ],
            axis=0,
        ).astype(jnp.bfloat16)
        for half in range(2)
    ]
    total = None
    for base in (0, 3):
        gate = upward = None
        for part in range(parts):
            size = buffers[base].shape[0] // parts
            span = slice(part * size, (part + 1) * size)
            every[base][part].wait()
            every[base + 1][part].wait()
            piece = pieces[part]
            gate_part = jnp.dot(
                piece, buffers[base][span, :], preferred_element_type=jnp.float32
            )
            up_part = jnp.dot(
                piece, buffers[base + 1][span, :], preferred_element_type=jnp.float32
            )
            gate = gate_part if gate is None else gate + gate_part
            upward = up_part if upward is None else upward + up_part
        hidden = (jax.nn.silu(gate) * upward).astype(jnp.bfloat16)
        for part in range(parts):
            every[base + 2][part].wait()
        out = jnp.dot(hidden, buffers[base + 2][...], preferred_element_type=jnp.float32)
        total = out if total is None else total + out
    total = total.astype(jnp.bfloat16)
    model = total.shape[1]
    for ref, rows in ((first_out_ref, total[:held]), (second_out_ref, total[held:])):
        ref[...] = sum(
            lax.dot_general(
                pick[half],
                rows[:, half * (model // 2) : (half + 1) * (model // 2)],
                (((0,), (0,)), ((), ())),
                preferred_element_type=jnp.float32,
            )
            for half in range(2)
        ).astype(jnp.bfloat16)


def partial_out(first, second, own, other, capacity):
    weights = (*own, *other)
    vmem = pl.BlockSpec(memory_space=pltpu.VMEM)
    out = jax.ShapeDtypeStruct(first.shape, jnp.bfloat16)
    return pl.pallas_call(
        functools.partial(experts_kernel, capacity),
        out_shape=(out, out),
        in_specs=[vmem] * 2 + [pl.BlockSpec(memory_space=pltpu.HBM)] * 6,
        scratch_shapes=[pltpu.VMEM(w.shape, w.dtype) for w in weights]
        + [pltpu.SemaphoreType.DMA((6, 2))],
        compiler_params=pltpu.CompilerParams(vmem_limit_bytes=56 << 20),
        name="experts",
    )(first, second, *weights)


def slot_numbers(route_rows, experts, capacity):
    flat = route_rows.reshape(route_rows.shape[:-2] + (-1,))
    matches = (flat[..., None] == jnp.arange(experts, dtype=jnp.int32)).astype(jnp.int32)
    earlier = jnp.cumsum(matches, axis=-2) - matches
    return flat * capacity + jnp.sum(earlier * matches, axis=-1)


def half_places(slots, capacity):
    first = slots // capacity * (2 * capacity) + slots % capacity
    return jnp.stack([first, first + capacity])


def dispatch_rows(places, normed, width):
    tokens, model = normed.shape
    hits = places[..., None] == jnp.arange(width, dtype=jnp.int32)
    hits = hits.astype(jnp.bfloat16).reshape(2, tokens, -1, width).sum(axis=2)
    halves = jnp.concatenate([normed[:, : model // 2], normed[:, model // 2 :]], axis=0)
    return jnp.einsum(
        "tw,td->wd", hits.reshape(2 * tokens, width), halves, preferred_element_type=jnp.float32
    ).astype(jnp.bfloat16)


def chip_shift(distance, flip=0):
    size = lax.axis_size("tp")
    chips = size // 2
    return [
        (2 * chip + core, 2 * ((chip + distance) % chips) + (core ^ flip))
        for chip in range(chips)
        for core in range(2)
    ]


def gathered_projection(out_proj, ends):
    chips = lax.axis_size("tp") // 2
    blocks = [
        lax.ppermute(out_proj, "tp", chip_shift(distance)) for distance in range(1, chips)
    ]
    *blocks, ends = lax.optimization_barrier((*blocks, ends))
    mine = jnp.concatenate([out_proj, *blocks], axis=0)
    other = lax.ppermute(mine, "tp", chip_shift(0, 1))
    return (mine, other), ends


def project_own(activated, wide_proj, own_rows):
    size = lax.axis_size("tp")
    chips = size // 2
    here = lax.axis_index("tp")
    chip, core = here // 2, here % 2
    arrived = lax.all_to_all(
        activated.reshape(size, own_rows, -1), "tp", split_axis=0, concat_axis=0, tiled=True
    )

    def parity_rows(parity):
        return jnp.concatenate(
            [
                lax.dynamic_index_in_dim(
                    arrived, 2 * ((chip - distance) % chips) + parity, 0, keepdims=False
                )
                for distance in range(chips)
            ],
            axis=1,
        )

    mine, other = wide_proj
    return jnp.dot(
        parity_rows(core), mine, preferred_element_type=jnp.float32
    ) + jnp.dot(parity_rows(1 - core), other, preferred_element_type=jnp.float32)


def expert_over_chips(rows, w_gate, w_up, w_down, capacity):
    rows, *sent = lax.optimization_barrier((rows, w_gate, w_up, w_down))
    before = lax.ppermute(rows, "tp", chip_shift(1))
    after = lax.ppermute(rows, "tp", chip_shift(-1))
    other = [lax.ppermute(w, "tp", chip_shift(0, 1)) for w in sent]
    late_rows, before, after = lax.optimization_barrier((rows, before, after))
    across = lax.ppermute(late_rows, "tp", chip_shift(2))
    own = (w_gate, w_up, w_down)
    for_before, for_after = partial_out(before, after, own, other, capacity)
    total, for_across = partial_out(rows, across, own, other, capacity)
    back = [
        lax.ppermute(for_before, "tp", chip_shift(-1)),
        lax.ppermute(for_after, "tp", chip_shift(1)),
        lax.ppermute(for_across, "tp", chip_shift(2)),
    ]
    total = total.astype(jnp.float32)
    for part in back:
        total = total + part.astype(jnp.float32)
    return total.astype(jnp.bfloat16)


def weighted_pick(places, weights, returned_result):
    width = returned_result.shape[0]
    tokens, top = weights.shape
    hits = places.reshape(2, tokens, top)[..., None] == jnp.arange(width, dtype=jnp.int32)
    spread = jnp.sum(jnp.where(hits, weights[None, :, :, None], 0.0), axis=2)
    spread = spread.reshape(2 * tokens, width)
    high = spread.astype(jnp.bfloat16)
    low = (spread - high.astype(jnp.float32)).astype(jnp.bfloat16)
    picked = jnp.dot(high, returned_result, preferred_element_type=jnp.float32) + jnp.dot(
        low, returned_result, preferred_element_type=jnp.float32
    )
    return jnp.concatenate([picked[:tokens], picked[tokens:]], axis=1)


def shards(
    mixer_input,
    decay_shift,
    pole_real,
    pole_imaginary,
    log_step,
    input_map,
    readout_matrix,
    skip,
    out_proj,
    stream,
    norm_gain,
    routes,
    route_logits,
    w_gate,
    w_up,
    w_down,
):
    rows = mixer_input.shape[0]
    totals, *kept = local_states(
        mixer_input,
        decay_shift,
        pole_real,
        pole_imaginary,
        log_step,
        input_map,
        lax.axis_size("sp"),
    )
    ends = lax.all_to_all(totals, "sp", split_axis=0, concat_axis=0, tiled=True)
    wide_proj, ends = gathered_projection(out_proj, ends)
    activated = activations(
        lax.axis_index("sp"), ends, kept, mixer_input, readout_matrix, skip
    )
    own_rows = rows // lax.axis_size("tp")
    model = stream.shape[1]
    projected = project_own(activated, wide_proj, own_rows)
    mixed = (stream.astype(jnp.float32) + projected).astype(jnp.bfloat16)
    mixed_wide = mixed.astype(jnp.float32)
    normed = (
        mixed_wide
        * lax.rsqrt(jnp.mean(mixed_wide * mixed_wide, axis=-1, keepdims=True) + EPS)
        * norm_gain
    ).astype(jnp.bfloat16)
    weights = jax.nn.sigmoid(
        jnp.stack(
            [route_logits[:, 0] - route_logits[:, 1], route_logits[:, 1] - route_logits[:, 0]],
            axis=1,
        )
    )
    experts = lax.axis_size("sp") * w_gate.shape[0]
    capacity = 4 * own_rows // experts
    width = 2 * experts * capacity
    places = half_places(slot_numbers(routes, experts, capacity), capacity)
    outgoing = dispatch_rows(places, normed, width)

    def over_experts(halves):
        blocks = halves.reshape(experts, 2 * capacity, model // 2)
        return lax.all_to_all(blocks, "sp", split_axis=0, concat_axis=0, tiled=True).reshape(
            width, model // 2
        )

    summed = expert_over_chips(over_experts(outgoing), w_gate[0], w_up[0], w_down[0], capacity)
    combined = mixed_wide + weighted_pick(places, weights, over_experts(summed))
    return combined.astype(jnp.bfloat16)


def solution(mesh):
    return jax.shard_map(
        shards,
        mesh=mesh,
        in_specs=(
            P("sp", "tp"),
            P("sp", "tp"),
            P("tp", None),
            P("tp", None),
            P("tp"),
            P(None, "tp", None, None),
            P(None, "tp", None, None),
            P("tp"),
            P("tp", None),
            P(("sp", "tp"), None),
            P(),
            P(("sp", "tp"), None),
            P(("sp", "tp"), None),
            P("sp", None, "tp"),
            P("sp", None, "tp"),
            P("sp", "tp", None),
        ),
        out_specs=P(("sp", "tp"), None),
        check_vma=False,
    )
```

```python
import functools

import jax
import jax.numpy as jnp
from jax import lax
from jax.experimental import pallas as pl
from jax.experimental.pallas import tpu as pltpu
from jax.sharding import PartitionSpec as P


EPS = 1e-06


LANES = 8
EXACT = lax.Precision.HIGHEST


def one_hot(shape, test):
    rows = lax.broadcasted_iota(jnp.int32, shape, 0)
    columns = lax.broadcasted_iota(jnp.int32, shape, 1)
    return jnp.where(test(rows, columns), 1.0, 0.0).astype(jnp.float32)


def exact_dot(left, right, transposed=False):
    contract = ((1,), (1,)) if transposed else ((1,), (0,))
    return lax.dot_general(
        left, right, (contract, ((), ())), precision=EXACT, preferred_element_type=jnp.float32
    )


def complex_times(a_real, a_imag, b_real, b_imag):
    return a_real * b_real - a_imag * b_imag, a_real * b_imag + a_imag * b_real


def states_kernel(
    input_hbm,
    shift_hbm,
    pole_real_hbm,
    pole_imag_hbm,
    log_step_hbm,
    map_hbm,
    total_ref,
    drive_real_ref,
    drive_imag_ref,
    scale_ref,
    factor_ref,
    enter_ref,
    input_ref,
    shift_ref,
    pole_real_ref,
    pole_imag_ref,
    log_step_ref,
    map_ref,
    semaphores,
):
    sources = (pole_real_hbm, pole_imag_hbm, log_step_hbm, shift_hbm, input_hbm, map_hbm)
    targets = (pole_real_ref, pole_imag_ref, log_step_ref, shift_ref, input_ref, map_ref)
    copies = [
        pltpu.make_async_copy(source, target, semaphores.at[number])
        for number, (source, target) in enumerate(zip(sources, targets))
    ]
    for copy in copies:
        copy.start()
    for copy in copies:
        copy.wait()
    rows = input_ref.shape[0]
    groups, states = pole_real_ref.shape
    width = groups * states
    channels = map_ref.shape[1] // groups
    length = rows // LANES
    spread = one_hot((states, width), lambda r, c: c % states == r)
    group_of = one_hot((groups, width), lambda r, c: c // states == r)

    def in_a_row(ref):
        return jnp.sum(exact_dot(ref[...], spread) * group_of, axis=0, keepdims=True)

    pole_real, pole_imag = in_a_row(pole_real_ref), in_a_row(pole_imag_ref)
    logs = jnp.broadcast_to(log_step_ref[...], (groups, groups))
    step = jnp.exp(exact_dot(logs, group_of)[:1])
    magnitude = jnp.exp(pole_real * step)
    factor_real = magnitude * jnp.cos(pole_imag * step)
    factor_imag = magnitude * jnp.sin(pole_imag * step)
    denominator = pole_real * pole_real + pole_imag * pole_imag
    ratio_real = ((factor_real - 1.0) * pole_real + factor_imag * pole_imag) / denominator
    ratio_imag = (factor_imag * pole_real - (factor_real - 1.0) * pole_imag) / denominator
    factor_ref[0:1, :] = factor_real
    factor_ref[1:2, :] = factor_imag

    order = one_hot((rows, rows), lambda r, c: c == (r % LANES) * length + r // LANES)
    inputs = jnp.dot(
        order.astype(jnp.bfloat16), input_ref[...], preferred_element_type=jnp.float32
    )
    scale_ref[...] = exact_dot(exact_dot(order, jnp.exp(shift_ref[...]), True), group_of)
    same_group = one_hot(
        (groups * channels, width), lambda r, c: r // channels == c // states
    )
    plain_real = exact_dot(inputs, exact_dot(map_ref[0], spread) * same_group)
    plain_imag = exact_dot(inputs, exact_dot(map_ref[1], spread) * same_group)
    drive_real, drive_imag = complex_times(ratio_real, ratio_imag, plain_real, plain_imag)
    drive_real_ref[...] = drive_real
    drive_imag_ref[...] = drive_imag

    wide_real = jnp.broadcast_to(factor_real, (LANES, width))
    wide_imag = jnp.broadcast_to(factor_imag, (LANES, width))
    through_real = jnp.ones((LANES, width), jnp.float32)
    through_imag = state_real = state_imag = jnp.zeros((LANES, width), jnp.float32)
    for k in range(length):
        at = slice(k * LANES, (k + 1) * LANES)
        scale = scale_ref[at, :]
        real, imag = scale * wide_real, scale * wide_imag
        through_real, through_imag = complex_times(real, imag, through_real, through_imag)
        state_real, state_imag = complex_times(real, imag, state_real, state_imag)
        state_real = state_real + drive_real_ref[at, :]
        state_imag = state_imag + drive_imag_ref[at, :]

    place = lax.broadcasted_iota(jnp.int32, (LANES, width), 0)

    def moved(value, by, empty):
        return jnp.where(place >= by, pltpu.roll(value, by, 0), empty)

    by = 1
    while by < LANES:
        a_real, a_imag = moved(through_real, by, 1.0), moved(through_imag, by, 0.0)
        x_real, x_imag = moved(state_real, by, 0.0), moved(state_imag, by, 0.0)
        x_real, x_imag = complex_times(through_real, through_imag, x_real, x_imag)
        state_real, state_imag = state_real + x_real, state_imag + x_imag
        through_real, through_imag = complex_times(through_real, through_imag, a_real, a_imag)
        by *= 2
    enter_ref[0] = moved(through_real, 1, 1.0)
    enter_ref[1] = moved(through_imag, 1, 0.0)
    enter_ref[2] = moved(state_real, 1, 0.0)
    enter_ref[3] = moved(state_imag, 1, 0.0)
    total = jnp.concatenate(
        [v[LANES - 1 :] for v in (through_real, through_imag, state_real, state_imag)], axis=0
    )
    total_ref[...] = jnp.broadcast_to(total[None], total_ref.shape)


def response_kernel(
    here_ref,
    arrived_ref,
    drive_real_ref,
    drive_imag_ref,
    scale_ref,
    factor_ref,
    enter_ref,
    input_ref,
    readout_ref,
    skip_ref,
    out_ref,
    state_ref,
):
    rows = input_ref.shape[0]
    width = factor_ref.shape[1]
    states = readout_ref.shape[2]
    channels = readout_ref.shape[1] * states // width
    length = rows // LANES
    here = here_ref[0]
    carry_real = carry_imag = jnp.zeros((1, width), jnp.float32)
    for j in range(arrived_ref.shape[0]):
        block = arrived_ref[j]
        real, imag = complex_times(block[0:1], block[1:2], carry_real, carry_imag)
        earlier = j < here
        carry_real = jnp.where(earlier, real + block[2:3], carry_real)
        carry_imag = jnp.where(earlier, imag + block[3:4], carry_imag)
    state_real, state_imag = complex_times(enter_ref[0], enter_ref[1], carry_real, carry_imag)
    state_real, state_imag = state_real + enter_ref[2], state_imag + enter_ref[3]
    wide_real = jnp.broadcast_to(factor_ref[0:1, :], (LANES, width))
    wide_imag = jnp.broadcast_to(factor_ref[1:2, :], (LANES, width))
    for k in range(length):
        at = slice(k * LANES, (k + 1) * LANES)
        scale = scale_ref[at, :]
        real, imag = scale * wide_real, scale * wide_imag
        state_real, state_imag = complex_times(real, imag, state_real, state_imag)
        state_real = state_real + drive_real_ref[at, :]
        state_imag = state_imag + drive_imag_ref[at, :]
        state_ref[at, :width] = state_real
        state_ref[at, width:] = state_imag
    spread = one_hot((states, width), lambda r, c: c % states == r)
    same_group = one_hot(
        (readout_ref.shape[1], width), lambda r, c: r // channels == c // states
    )
    matrix = jnp.concatenate(
        [
            exact_dot(readout_ref[0], spread) * same_group,
            exact_dot(readout_ref[1], spread) * -same_group,
        ],
        axis=1,
    )
    response = exact_dot(state_ref[...], matrix, True)
    order = one_hot((rows, rows), lambda r, c: r == (c % LANES) * length + c // LANES)
    response = exact_dot(order, response) + skip_ref[...] * input_ref[...].astype(jnp.float32)
    out_ref[...] = jax.nn.gelu(response).astype(jnp.bfloat16)


def local_states(
    mixer_input, decay_shift, pole_real, pole_imaginary, log_step, input_map, devices
):
    rows = mixer_input.shape[0]
    groups, states = pole_real.shape
    width = groups * states
    f32 = jnp.float32
    shape = jax.ShapeDtypeStruct
    operands = (
        mixer_input,
        decay_shift.T,
        pole_real,
        pole_imaginary,
        log_step[None],
        jnp.swapaxes(input_map, 2, 3).reshape(2, -1, states),
    )
    return pl.pallas_call(
        states_kernel,
        out_shape=(
            shape((devices, 4, width), f32),
            shape((rows, width), f32),
            shape((rows, width), f32),
            shape((rows, width), f32),
            shape((2, width), f32),
            shape((4, LANES, width), f32),
        ),
        in_specs=[pl.BlockSpec(memory_space=pltpu.HBM)] * len(operands),
        scratch_shapes=[pltpu.VMEM(operand.shape, operand.dtype) for operand in operands]
        + [pltpu.SemaphoreType.DMA((len(operands),))],
        compiler_params=pltpu.CompilerParams(vmem_limit_bytes=60 * 1024 * 1024),
        name="states",
    )(*operands)


def activations(here, arrived, kept, mixer_input, readout_matrix, skip):
    rows, channels = mixer_input.shape
    width = arrived.shape[2]
    vmem = pl.BlockSpec(memory_space=pltpu.VMEM)
    return pl.pallas_call(
        response_kernel,
        out_shape=jax.ShapeDtypeStruct((rows, channels), jnp.bfloat16),
        in_specs=[pl.BlockSpec(memory_space=pltpu.SMEM)] + [vmem] * 9,
        scratch_shapes=[pltpu.VMEM((rows, 2 * width), jnp.float32)],
        compiler_params=pltpu.CompilerParams(vmem_limit_bytes=60 * 1024 * 1024),
        name="response",
    )(
        here.reshape(1),
        arrived,
        *kept,
        mixer_input,
        readout_matrix.reshape(2, channels, -1),
        skip[None],
    )


def experts_kernel(capacity, count, sets, resumed, finished, *refs):
    row_refs, refs = refs[:count], refs[count:]
    weights, refs = refs[: 3 * sets], refs[3 * sets :]
    before, outs = (refs[:count], refs[count:]) if resumed else ((), refs)
    held, part = row_refs[0].shape[0] // 2, row_refs[0].shape[1]

    def whole_rows(half):
        return one_hot(
            (held, 2 * held),
            lambda r, c: c == r // capacity * (2 * capacity) + r % capacity + half * capacity,
        ).astype(jnp.bfloat16)

    pick = [whole_rows(half) for half in range(2)]
    pieces = [
        jnp.concatenate(
            [jnp.dot(chosen, ref[...], preferred_element_type=jnp.float32) for ref in row_refs],
            axis=0,
        ).astype(jnp.bfloat16)
        for chosen in pick
    ]
    total = jnp.concatenate([ref[...] for ref in before], axis=0) if resumed else None
    for number in range(sets):
        gate_ref, up_ref, down_ref = weights[3 * number : 3 * number + 3]

        def product(ref):
            return sum(
                jnp.dot(
                    piece,
                    ref[half * part : (half + 1) * part, :],
                    preferred_element_type=jnp.float32,
                )
                for half, piece in enumerate(pieces)
            )

        hidden = (jax.nn.silu(product(gate_ref)) * product(up_ref)).astype(jnp.bfloat16)
        out = jnp.dot(hidden, down_ref[...], preferred_element_type=jnp.float32)
        total = out if total is None else total + out
    for number, ref in enumerate(outs):
        rows = total[number * held : (number + 1) * held]
        if finished:
            rows = rows.astype(jnp.bfloat16)
            rows = sum(
                lax.dot_general(
                    pick[half],
                    rows[:, half * part : (half + 1) * part],
                    (((0,), (0,)), ((), ())),
                    preferred_element_type=jnp.float32,
                )
                for half in range(2)
            ).astype(jnp.bfloat16)
        ref[...] = rows


def partial_out(rows, weights, capacity, resumed=(), finished=True):
    count, sets = len(rows), len(weights) // 3
    halves, part = rows[0].shape
    if finished:
        out = jax.ShapeDtypeStruct((halves, part), jnp.bfloat16)
    else:
        out = jax.ShapeDtypeStruct((halves // 2, 2 * part), jnp.float32)
    kernel = functools.partial(
        experts_kernel, capacity, count, sets, bool(resumed), finished
    )
    flops = 2 * count * (halves // 2) * sum(w.size for w in weights)
    return pl.pallas_call(
        kernel,
        out_shape=(out,) * count,
        in_specs=[pl.BlockSpec(memory_space=pltpu.VMEM)]
        * (count + len(weights) + len(resumed)),
        compiler_params=pltpu.CompilerParams(vmem_limit_bytes=20 << 20),
        cost_estimate=pl.CostEstimate(flops=flops, bytes_accessed=0, transcendentals=0),
        name="experts",
    )(*rows, *weights, *resumed)


def slot_numbers(route_rows, experts, capacity):
    flat = route_rows.reshape(route_rows.shape[:-2] + (-1,))
    matches = (flat[..., None] == jnp.arange(experts, dtype=jnp.int32)).astype(jnp.int32)
    earlier = jnp.cumsum(matches, axis=-2) - matches
    return flat * capacity + jnp.sum(earlier * matches, axis=-1)


def half_places(slots, capacity):
    first = slots // capacity * (2 * capacity) + slots % capacity
    return jnp.stack([first, first + capacity])


def chip_shift(distance, flip=0):
    size = lax.axis_size("tp")
    chips = size // 2
    return [
        (2 * chip + core, 2 * ((chip + distance) % chips) + (core ^ flip))
        for chip in range(chips)
        for core in range(2)
    ]


def gathered_projection(out_proj):
    chips = lax.axis_size("tp") // 2
    mine = [out_proj] + [
        lax.ppermute(out_proj, "tp", chip_shift(distance)) for distance in range(1, chips)
    ]
    other = [lax.ppermute(block, "tp", chip_shift(0, 1)) for block in mine]
    return (*mine, *other)


def mix_kernel(order_ref, arrived_ref, stream_ref, gain_ref, places_ref, *refs):
    *blocks, mixed_ref, outgoing_ref = refs
    tokens, model = stream_ref.shape
    projected = sum(
        jnp.dot(arrived_ref[order_ref[number]], block[...], preferred_element_type=jnp.float32)
        for number, block in enumerate(blocks)
    )
    mixed = (stream_ref[...].astype(jnp.float32) + projected).astype(jnp.bfloat16)
    mixed_ref[...] = mixed
    wide = mixed.astype(jnp.float32)
    mean = jnp.mean(wide * wide, axis=-1, keepdims=True)
    normed = (wide * lax.rsqrt(mean + EPS) * gain_ref[...]).astype(jnp.bfloat16)
    halves = jnp.concatenate([normed[:, : model // 2], normed[:, model // 2 :]], axis=0)
    width = outgoing_ref.shape[0]
    at = lax.broadcasted_iota(jnp.int32, (2 * tokens, width), 1)
    hits = sum(
        jnp.where(at == places_ref[:, k : k + 1], 1.0, 0.0) for k in range(places_ref.shape[1])
    ).astype(jnp.bfloat16)
    outgoing_ref[...] = lax.dot_general(
        hits, halves, (((0,), (0,)), ((), ())), preferred_element_type=jnp.float32
    ).astype(jnp.bfloat16)


def mixed_and_outgoing(activated, blocks, stream, norm_gain, places, width):
    size = lax.axis_size("tp")
    chips = size // 2
    here = lax.axis_index("tp")
    chip, core = here // 2, here % 2
    tokens, model = stream.shape
    back = 2 * ((chip - jnp.arange(chips, dtype=jnp.int32)) % chips)
    order = jnp.concatenate([back + core, back + 1 - core])
    arrived = lax.all_to_all(
        activated.reshape(size, tokens, -1), "tp", split_axis=0, concat_axis=0, tiled=True
    )
    vmem = pl.BlockSpec(memory_space=pltpu.VMEM)
    shape = jax.ShapeDtypeStruct
    return pl.pallas_call(
        mix_kernel,
        out_shape=(
            shape((tokens, model), jnp.bfloat16),
            shape((width, model // 2), jnp.bfloat16),
        ),
        in_specs=[pl.BlockSpec(memory_space=pltpu.SMEM)]
        + [vmem] * (4 + size),
        compiler_params=pltpu.CompilerParams(vmem_limit_bytes=12 << 20),
        name="mix",
    )(order, arrived, stream, norm_gain[None], places.reshape(2 * tokens, -1), *blocks)


def expert_over_chips(rows, w_gate, w_up, w_down, capacity):
    own = (w_gate, w_up, w_down)
    rows, *sent = lax.optimization_barrier((rows, *own))
    before = lax.ppermute(rows, "tp", chip_shift(1))
    after = lax.ppermute(rows, "tp", chip_shift(-1))
    other = [lax.ppermute(w, "tp", chip_shift(0, 1)) for w in sent]
    (kept,) = partial_out((rows,), own, capacity, finished=False)
    before, after, kept, late_rows = lax.optimization_barrier((before, after, kept, rows))
    across = lax.ppermute(late_rows, "tp", chip_shift(2))
    near = partial_out((before, after), own, capacity, finished=False)
    for_before, for_after = partial_out((before, after), other, capacity, near)
    (total,) = partial_out((rows,), other, capacity, (kept,))
    (for_across,) = partial_out((across,), (*own, *other), capacity)
    total = total.astype(jnp.float32)
    total = total + lax.ppermute(for_before, "tp", chip_shift(-1)).astype(jnp.float32)
    total = total + lax.ppermute(for_after, "tp", chip_shift(1)).astype(jnp.float32)
    total = lax.optimization_barrier(total)
    total = total + lax.ppermute(for_across, "tp", chip_shift(2)).astype(jnp.float32)
    return total.astype(jnp.bfloat16)


def weighted_pick(places, weights, returned_result):
    width = returned_result.shape[0]
    tokens, top = weights.shape
    hits = places.reshape(2, tokens, top)[..., None] == jnp.arange(width, dtype=jnp.int32)
    spread = jnp.sum(jnp.where(hits, weights[None, :, :, None], 0.0), axis=2)
    spread = spread.reshape(2 * tokens, width)
    high = spread.astype(jnp.bfloat16)
    low = (spread - high.astype(jnp.float32)).astype(jnp.bfloat16)
    picked = jnp.dot(high, returned_result, preferred_element_type=jnp.float32) + jnp.dot(
        low, returned_result, preferred_element_type=jnp.float32
    )
    return jnp.concatenate([picked[:tokens], picked[tokens:]], axis=1)


def shards(
    mixer_input,
    decay_shift,
    pole_real,
    pole_imaginary,
    log_step,
    input_map,
    readout_matrix,
    skip,
    out_proj,
    stream,
    norm_gain,
    routes,
    route_logits,
    w_gate,
    w_up,
    w_down,
):
    totals, *kept = local_states(
        mixer_input,
        decay_shift,
        pole_real,
        pole_imaginary,
        log_step,
        input_map,
        lax.axis_size("sp"),
    )
    ends = lax.all_to_all(totals, "sp", split_axis=0, concat_axis=0, tiled=True)
    blocks = gathered_projection(out_proj)
    activated = activations(
        lax.axis_index("sp"), ends, kept, mixer_input, readout_matrix, skip
    )
    own_rows, model = stream.shape
    weights = jax.nn.sigmoid(
        jnp.stack(
            [route_logits[:, 0] - route_logits[:, 1], route_logits[:, 1] - route_logits[:, 0]],
            axis=1,
        )
    )
    experts = lax.axis_size("sp") * w_gate.shape[0]
    capacity = 4 * own_rows // experts
    width = 2 * experts * capacity
    places = half_places(slot_numbers(routes, experts, capacity), capacity)
    mixed, outgoing = mixed_and_outgoing(
        activated, blocks, stream, norm_gain, places, width
    )
    mixed_wide = mixed.astype(jnp.float32)

    def over_experts(halves):
        blocks = halves.reshape(experts, 2 * capacity, model // 2)
        return lax.all_to_all(blocks, "sp", split_axis=0, concat_axis=0, tiled=True).reshape(
            width, model // 2
        )

    summed = expert_over_chips(over_experts(outgoing), w_gate[0], w_up[0], w_down[0], capacity)
    combined = mixed_wide + weighted_pick(places, weights, over_experts(summed))
    return combined.astype(jnp.bfloat16)


def solution(mesh):
    return jax.shard_map(
        shards,
        mesh=mesh,
        in_specs=(
            P("sp", "tp"),
            P("sp", "tp"),
            P("tp", None),
            P("tp", None),
            P("tp"),
            P(None, "tp", None, None),
            P(None, "tp", None, None),
            P("tp"),
            P("tp", None),
            P(("sp", "tp"), None),
            P(),
            P(("sp", "tp"), None),
            P(("sp", "tp"), None),
            P("sp", None, "tp"),
            P("sp", None, "tp"),
            P("sp", "tp", None),
        ),
        out_specs=P(("sp", "tp"), None),
        check_vma=False,
    )
```

```python
import functools

import jax
import jax.numpy as jnp
from jax import lax
from jax.experimental import pallas as pl
from jax.experimental.pallas import tpu as pltpu
from jax.sharding import PartitionSpec as P


EPS = 1e-06


LANES = 8
EXACT = lax.Precision.HIGHEST


def one_hot(shape, test):
    rows = lax.broadcasted_iota(jnp.int32, shape, 0)
    columns = lax.broadcasted_iota(jnp.int32, shape, 1)
    return jnp.where(test(rows, columns), 1.0, 0.0).astype(jnp.float32)


def exact_dot(left, right, transposed=False):
    contract = ((1,), (1,)) if transposed else ((1,), (0,))
    return lax.dot_general(
        left, right, (contract, ((), ())), precision=EXACT, preferred_element_type=jnp.float32
    )


def complex_times(a_real, a_imag, b_real, b_imag):
    return a_real * b_real - a_imag * b_imag, a_real * b_imag + a_imag * b_real


def states_kernel(
    input_hbm,
    shift_hbm,
    pole_real_hbm,
    pole_imag_hbm,
    log_step_hbm,
    map_hbm,
    total_ref,
    drive_real_ref,
    drive_imag_ref,
    scale_ref,
    factor_ref,
    enter_ref,
    input_ref,
    shift_ref,
    pole_real_ref,
    pole_imag_ref,
    log_step_ref,
    map_ref,
    semaphores,
):
    sources = (pole_real_hbm, pole_imag_hbm, log_step_hbm, shift_hbm, input_hbm, map_hbm)
    targets = (pole_real_ref, pole_imag_ref, log_step_ref, shift_ref, input_ref, map_ref)
    copies = [
        pltpu.make_async_copy(source, target, semaphores.at[number])
        for number, (source, target) in enumerate(zip(sources, targets))
    ]
    for copy in copies:
        copy.start()
    for copy in copies:
        copy.wait()
    rows = input_ref.shape[0]
    groups, states = pole_real_ref.shape
    width = groups * states
    channels = map_ref.shape[1] // groups
    length = rows // LANES
    spread = one_hot((states, width), lambda r, c: c % states == r)
    group_of = one_hot((groups, width), lambda r, c: c // states == r)

    def in_a_row(ref):
        return jnp.sum(exact_dot(ref[...], spread) * group_of, axis=0, keepdims=True)

    pole_real, pole_imag = in_a_row(pole_real_ref), in_a_row(pole_imag_ref)
    logs = jnp.broadcast_to(log_step_ref[...], (groups, groups))
    step = jnp.exp(exact_dot(logs, group_of)[:1])
    magnitude = jnp.exp(pole_real * step)
    factor_real = magnitude * jnp.cos(pole_imag * step)
    factor_imag = magnitude * jnp.sin(pole_imag * step)
    denominator = pole_real * pole_real + pole_imag * pole_imag
    ratio_real = ((factor_real - 1.0) * pole_real + factor_imag * pole_imag) / denominator
    ratio_imag = (factor_imag * pole_real - (factor_real - 1.0) * pole_imag) / denominator
    factor_ref[0:1, :] = factor_real
    factor_ref[1:2, :] = factor_imag

    order = one_hot((rows, rows), lambda r, c: c == (r % LANES) * length + r // LANES)
    inputs = jnp.dot(
        order.astype(jnp.bfloat16), input_ref[...], preferred_element_type=jnp.float32
    )
    scale_ref[...] = exact_dot(exact_dot(order, jnp.exp(shift_ref[...]), True), group_of)
    same_group = one_hot(
        (groups * channels, width), lambda r, c: r // channels == c // states
    )
    plain_real = exact_dot(inputs, exact_dot(map_ref[0], spread) * same_group)
    plain_imag = exact_dot(inputs, exact_dot(map_ref[1], spread) * same_group)
    drive_real, drive_imag = complex_times(ratio_real, ratio_imag, plain_real, plain_imag)
    drive_real_ref[...] = drive_real
    drive_imag_ref[...] = drive_imag

    wide_real = jnp.broadcast_to(factor_real, (LANES, width))
    wide_imag = jnp.broadcast_to(factor_imag, (LANES, width))
    through_real = jnp.ones((LANES, width), jnp.float32)
    through_imag = state_real = state_imag = jnp.zeros((LANES, width), jnp.float32)
    for k in range(length):
        at = slice(k * LANES, (k + 1) * LANES)
        scale = scale_ref[at, :]
        real, imag = scale * wide_real, scale * wide_imag
        through_real, through_imag = complex_times(real, imag, through_real, through_imag)
        state_real, state_imag = complex_times(real, imag, state_real, state_imag)
        state_real = state_real + drive_real_ref[at, :]
        state_imag = state_imag + drive_imag_ref[at, :]

    place = lax.broadcasted_iota(jnp.int32, (LANES, width), 0)

    def moved(value, by, empty):
        return jnp.where(place >= by, pltpu.roll(value, by, 0), empty)

    by = 1
    while by < LANES:
        a_real, a_imag = moved(through_real, by, 1.0), moved(through_imag, by, 0.0)
        x_real, x_imag = moved(state_real, by, 0.0), moved(state_imag, by, 0.0)
        x_real, x_imag = complex_times(through_real, through_imag, x_real, x_imag)
        state_real, state_imag = state_real + x_real, state_imag + x_imag
        through_real, through_imag = complex_times(through_real, through_imag, a_real, a_imag)
        by *= 2
    enter_ref[0] = moved(through_real, 1, 1.0)
    enter_ref[1] = moved(through_imag, 1, 0.0)
    enter_ref[2] = moved(state_real, 1, 0.0)
    enter_ref[3] = moved(state_imag, 1, 0.0)
    total = jnp.concatenate(
        [v[LANES - 1 :] for v in (through_real, through_imag, state_real, state_imag)], axis=0
    )
    total_ref[...] = jnp.broadcast_to(total[None], total_ref.shape)


def response_kernel(here_ref, *refs):
    sources, (out_ref, state_ref), targets, semaphores = (
        refs[:9],
        refs[9:11],
        refs[11:20],
        refs[20],
    )
    copies = [
        pltpu.make_async_copy(source, target, semaphores.at[number])
        for number, (source, target) in enumerate(zip(sources, targets))
    ]
    for copy in copies:
        copy.start()
    (
        arrived_ref,
        drive_real_ref,
        drive_imag_ref,
        scale_ref,
        factor_ref,
        enter_ref,
        input_ref,
        readout_ref,
        skip_ref,
    ) = targets
    copies[0].wait()
    rows = input_ref.shape[0]
    width = factor_ref.shape[1]
    states = readout_ref.shape[2]
    channels = readout_ref.shape[1] * states // width
    length = rows // LANES
    here = here_ref[0]
    carry_real = carry_imag = jnp.zeros((1, width), jnp.float32)
    for j in range(arrived_ref.shape[0]):
        block = arrived_ref[j]
        real, imag = complex_times(block[0:1], block[1:2], carry_real, carry_imag)
        earlier = j < here
        carry_real = jnp.where(earlier, real + block[2:3], carry_real)
        carry_imag = jnp.where(earlier, imag + block[3:4], carry_imag)
    for copy in copies[1:]:
        copy.wait()
    state_real, state_imag = complex_times(enter_ref[0], enter_ref[1], carry_real, carry_imag)
    state_real, state_imag = state_real + enter_ref[2], state_imag + enter_ref[3]
    wide_real = jnp.broadcast_to(factor_ref[0:1, :], (LANES, width))
    wide_imag = jnp.broadcast_to(factor_ref[1:2, :], (LANES, width))
    for k in range(length):
        at = slice(k * LANES, (k + 1) * LANES)
        scale = scale_ref[at, :]
        real, imag = scale * wide_real, scale * wide_imag
        state_real, state_imag = complex_times(real, imag, state_real, state_imag)
        state_real = state_real + drive_real_ref[at, :]
        state_imag = state_imag + drive_imag_ref[at, :]
        state_ref[at, :width] = state_real
        state_ref[at, width:] = state_imag
    spread = one_hot((states, width), lambda r, c: c % states == r)
    same_group = one_hot(
        (readout_ref.shape[1], width), lambda r, c: r // channels == c // states
    )
    matrix = jnp.concatenate(
        [
            exact_dot(readout_ref[0], spread) * same_group,
            exact_dot(readout_ref[1], spread) * -same_group,
        ],
        axis=1,
    )
    response = exact_dot(state_ref[...], matrix, True)
    order = one_hot((rows, rows), lambda r, c: r == (c % LANES) * length + c // LANES)
    response = exact_dot(order, response) + skip_ref[...] * input_ref[...].astype(jnp.float32)
    out_ref[...] = jax.nn.gelu(response).astype(jnp.bfloat16)


def local_states(
    mixer_input, decay_shift, pole_real, pole_imaginary, log_step, input_map, devices
):
    rows = mixer_input.shape[0]
    groups, states = pole_real.shape
    width = groups * states
    f32 = jnp.float32
    shape = jax.ShapeDtypeStruct
    operands = (
        mixer_input,
        decay_shift.T,
        pole_real,
        pole_imaginary,
        log_step[None],
        jnp.swapaxes(input_map, 2, 3).reshape(2, -1, states),
    )
    return pl.pallas_call(
        states_kernel,
        out_shape=(
            shape((devices, 4, width), f32),
            shape((rows, width), f32),
            shape((rows, width), f32),
            shape((rows, width), f32),
            shape((2, width), f32),
            shape((4, LANES, width), f32),
        ),
        in_specs=[pl.BlockSpec(memory_space=pltpu.HBM)] * len(operands),
        scratch_shapes=[pltpu.VMEM(operand.shape, operand.dtype) for operand in operands]
        + [pltpu.SemaphoreType.DMA((len(operands),))],
        compiler_params=pltpu.CompilerParams(vmem_limit_bytes=60 * 1024 * 1024),
        name="states",
    )(*operands)


def activations(here, arrived, kept, mixer_input, readout_matrix, skip):
    rows, channels = mixer_input.shape
    width = arrived.shape[2]
    operands = (
        arrived,
        *kept,
        mixer_input,
        readout_matrix.reshape(2, channels, -1),
        skip[None],
    )
    return pl.pallas_call(
        response_kernel,
        out_shape=jax.ShapeDtypeStruct((rows, channels), jnp.bfloat16),
        in_specs=[pl.BlockSpec(memory_space=pltpu.SMEM)]
        + [pl.BlockSpec(memory_space=pltpu.HBM)] * len(operands),
        scratch_shapes=[pltpu.VMEM((rows, 2 * width), jnp.float32)]
        + [pltpu.VMEM(operand.shape, operand.dtype) for operand in operands]
        + [pltpu.SemaphoreType.DMA((len(operands),))],
        compiler_params=pltpu.CompilerParams(vmem_limit_bytes=60 * 1024 * 1024),
        name="response",
    )(here.reshape(1), *operands)


def experts_kernel(capacity, count, sets, resumed, finished, *refs):
    row_refs, refs = refs[:count], refs[count:]
    weights, refs = refs[: 3 * sets], refs[3 * sets :]
    before, outs = (refs[:count], refs[count:]) if resumed else ((), refs)
    held, part = row_refs[0].shape[0] // 2, row_refs[0].shape[1]

    def whole_rows(half):
        return one_hot(
            (held, 2 * held),
            lambda r, c: c == r // capacity * (2 * capacity) + r % capacity + half * capacity,
        ).astype(jnp.bfloat16)

    pick = [whole_rows(half) for half in range(2)]
    pieces = [
        jnp.concatenate(
            [jnp.dot(chosen, ref[...], preferred_element_type=jnp.float32) for ref in row_refs],
            axis=0,
        ).astype(jnp.bfloat16)
        for chosen in pick
    ]
    total = jnp.concatenate([ref[...] for ref in before], axis=0) if resumed else None
    for number in range(sets):
        gate_ref, up_ref, down_ref = weights[3 * number : 3 * number + 3]

        def product(ref):
            return sum(
                jnp.dot(
                    piece,
                    ref[half * part : (half + 1) * part, :],
                    preferred_element_type=jnp.float32,
                )
                for half, piece in enumerate(pieces)
            )

        hidden = (jax.nn.silu(product(gate_ref)) * product(up_ref)).astype(jnp.bfloat16)
        out = jnp.dot(hidden, down_ref[...], preferred_element_type=jnp.float32)
        total = out if total is None else total + out
    for number, ref in enumerate(outs):
        rows = total[number * held : (number + 1) * held]
        if finished:
            rows = rows.astype(jnp.bfloat16)
            rows = sum(
                lax.dot_general(
                    pick[half],
                    rows[:, half * part : (half + 1) * part],
                    (((0,), (0,)), ((), ())),
                    preferred_element_type=jnp.float32,
                )
                for half in range(2)
            ).astype(jnp.bfloat16)
        ref[...] = rows


def partial_out(rows, weights, capacity, resumed=(), finished=True):
    count, sets = len(rows), len(weights) // 3
    halves, part = rows[0].shape
    if finished:
        out = jax.ShapeDtypeStruct((halves, part), jnp.bfloat16)
    else:
        out = jax.ShapeDtypeStruct((halves // 2, 2 * part), jnp.float32)
    kernel = functools.partial(
        experts_kernel, capacity, count, sets, bool(resumed), finished
    )
    flops = 2 * count * (halves // 2) * sum(w.size for w in weights)
    return pl.pallas_call(
        kernel,
        out_shape=(out,) * count,
        in_specs=[pl.BlockSpec(memory_space=pltpu.VMEM)]
        * (count + len(weights) + len(resumed)),
        compiler_params=pltpu.CompilerParams(vmem_limit_bytes=12 << 20),
        cost_estimate=pl.CostEstimate(flops=flops, bytes_accessed=0, transcendentals=0),
        name="experts",
    )(*rows, *weights, *resumed)


def slot_numbers(route_rows, experts, capacity):
    flat = route_rows.reshape(route_rows.shape[:-2] + (-1,))
    matches = (flat[..., None] == jnp.arange(experts, dtype=jnp.int32)).astype(jnp.int32)
    earlier = jnp.cumsum(matches, axis=-2) - matches
    return flat * capacity + jnp.sum(earlier * matches, axis=-1)


def half_places(slots, capacity):
    first = slots // capacity * (2 * capacity) + slots % capacity
    return jnp.stack([first, first + capacity])


def chip_shift(distance, flip=0):
    size = lax.axis_size("tp")
    chips = size // 2
    return [
        (2 * chip + core, 2 * ((chip + distance) % chips) + (core ^ flip))
        for chip in range(chips)
        for core in range(2)
    ]


def gathered_projection(out_proj):
    chips = lax.axis_size("tp") // 2
    mine = [out_proj] + [
        lax.ppermute(out_proj, "tp", chip_shift(distance)) for distance in range(1, chips)
    ]
    other = [lax.ppermute(block, "tp", chip_shift(0, 1)) for block in mine]
    return (*mine, *other)


def mix_kernel(order_ref, arrived_ref, stream_ref, gain_ref, places_ref, *refs):
    *blocks, mixed_ref, outgoing_ref = refs
    tokens, model = stream_ref.shape
    projected = sum(
        jnp.dot(arrived_ref[order_ref[number]], block[...], preferred_element_type=jnp.float32)
        for number, block in enumerate(blocks)
    )
    mixed = (stream_ref[...].astype(jnp.float32) + projected).astype(jnp.bfloat16)
    mixed_ref[...] = mixed
    wide = mixed.astype(jnp.float32)
    mean = jnp.mean(wide * wide, axis=-1, keepdims=True)
    normed = (wide * lax.rsqrt(mean + EPS) * gain_ref[...]).astype(jnp.bfloat16)
    halves = jnp.concatenate([normed[:, : model // 2], normed[:, model // 2 :]], axis=0)
    width = outgoing_ref.shape[0]
    at = lax.broadcasted_iota(jnp.int32, (2 * tokens, width), 1)
    hits = sum(
        jnp.where(at == places_ref[:, k : k + 1], 1.0, 0.0) for k in range(places_ref.shape[1])
    ).astype(jnp.bfloat16)
    outgoing_ref[...] = lax.dot_general(
        hits, halves, (((0,), (0,)), ((), ())), preferred_element_type=jnp.float32
    ).astype(jnp.bfloat16)


def mixed_and_outgoing(activated, blocks, stream, norm_gain, places, width):
    size = lax.axis_size("tp")
    chips = size // 2
    here = lax.axis_index("tp")
    chip, core = here // 2, here % 2
    tokens, model = stream.shape
    back = 2 * ((chip - jnp.arange(chips, dtype=jnp.int32)) % chips)
    order = jnp.concatenate([back + core, back + 1 - core])
    arrived = lax.all_to_all(
        activated.reshape(size, tokens, -1), "tp", split_axis=0, concat_axis=0, tiled=True
    )
    vmem = pl.BlockSpec(memory_space=pltpu.VMEM)
    shape = jax.ShapeDtypeStruct
    return pl.pallas_call(
        mix_kernel,
        out_shape=(
            shape((tokens, model), jnp.bfloat16),
            shape((width, model // 2), jnp.bfloat16),
        ),
        in_specs=[pl.BlockSpec(memory_space=pltpu.SMEM)]
        + [vmem] * (4 + size),
        compiler_params=pltpu.CompilerParams(vmem_limit_bytes=12 << 20),
        name="mix",
    )(order, arrived, stream, norm_gain[None], places.reshape(2 * tokens, -1), *blocks)


def over_experts(halves, experts):
    blocks = halves.reshape(experts, -1, halves.shape[1])
    return lax.all_to_all(blocks, "sp", split_axis=0, concat_axis=0, tiled=True).reshape(
        halves.shape
    )


def expert_over_chips(rows, w_gate, w_up, w_down, w_down_other, capacity):
    own = (w_gate, w_up, w_down)
    rows, *sent = lax.optimization_barrier((rows, w_gate, w_up))
    before = lax.ppermute(rows, "tp", chip_shift(1))
    after = lax.ppermute(rows, "tp", chip_shift(-1))
    other = [lax.ppermute(w, "tp", chip_shift(0, 1)) for w in sent] + [w_down_other]
    (kept,) = partial_out((rows,), own, capacity, finished=False)
    before, after, kept = lax.optimization_barrier((before, after, kept))
    middle = rows.shape[0] // 2
    across = (
        lax.ppermute(before[:middle], "tp", chip_shift(1)),
        lax.ppermute(after[middle:], "tp", chip_shift(-1)),
    )
    near = partial_out((before, after), own, capacity, finished=False)
    for_before, for_after = partial_out((before, after), other, capacity, near)
    to_before = lax.ppermute(for_before, "tp", chip_shift(-1))
    to_after = lax.ppermute(for_after, "tp", chip_shift(1))
    across, for_before = lax.optimization_barrier((across, for_before))
    for_across = partial_out(across, (*own, *other), capacity)
    to_across = [lax.ppermute(part, "tp", chip_shift(2)) for part in for_across]
    rows, _ = lax.optimization_barrier((rows, for_across))
    (total,) = partial_out((rows,), other, capacity, (kept,))
    total = total.astype(jnp.float32) + to_before.astype(jnp.float32)
    total = lax.optimization_barrier(total + to_after.astype(jnp.float32))
    total = total + jnp.concatenate(to_across, axis=0).astype(jnp.float32)
    return total.astype(jnp.bfloat16)


def spread_weights(places, weights, width):
    tokens, top = weights.shape
    hits = places.reshape(2, tokens, top)[..., None] == jnp.arange(width, dtype=jnp.int32)
    spread = jnp.sum(jnp.where(hits, weights[None, :, :, None], 0.0), axis=2)
    spread = spread.reshape(2 * tokens, width)
    high = spread.astype(jnp.bfloat16)
    return jnp.concatenate([high, (spread - high.astype(jnp.float32)).astype(jnp.bfloat16)])


def weighted_pick(spread, returned_result):
    parts = jnp.dot(spread, returned_result, preferred_element_type=jnp.float32)
    return parts[: len(parts) // 2] + parts[len(parts) // 2 :]


def shards(
    mixer_input,
    decay_shift,
    pole_real,
    pole_imaginary,
    log_step,
    input_map,
    readout_matrix,
    skip,
    out_proj,
    stream,
    norm_gain,
    routes,
    route_logits,
    w_gate,
    w_up,
    w_down,
):
    w_down_other = lax.ppermute(w_down[0], "tp", chip_shift(0, 1))
    totals, *kept = local_states(
        mixer_input,
        decay_shift,
        pole_real,
        pole_imaginary,
        log_step,
        input_map,
        lax.axis_size("sp"),
    )
    ends = lax.all_to_all(totals, "sp", split_axis=0, concat_axis=0, tiled=True)
    blocks = gathered_projection(out_proj)
    own_rows, _ = stream.shape
    weights = jax.nn.sigmoid(
        jnp.stack(
            [route_logits[:, 0] - route_logits[:, 1], route_logits[:, 1] - route_logits[:, 0]],
            axis=1,
        )
    )
    experts = lax.axis_size("sp") * w_gate.shape[0]
    capacity = 4 * own_rows // experts
    width = 2 * experts * capacity
    places = half_places(slot_numbers(routes, experts, capacity), capacity)
    spread = spread_weights(places, weights, width)
    ends, spread, places = lax.optimization_barrier((ends, spread, places))
    activated = activations(
        lax.axis_index("sp"), ends, kept, mixer_input, readout_matrix, skip
    )
    mixed, outgoing = mixed_and_outgoing(
        activated, blocks, stream, norm_gain, places, width
    )
    mixed_wide = mixed.astype(jnp.float32)

    arrived = over_experts(outgoing, experts)
    summed = expert_over_chips(
        arrived, w_gate[0], w_up[0], w_down[0], w_down_other, capacity
    )
    picked = weighted_pick(spread, over_experts(summed, experts))
    picked = jnp.concatenate([picked[:own_rows], picked[own_rows:]], axis=1)
    return (mixed_wide + picked).astype(jnp.bfloat16)


def solution(mesh):
    return jax.shard_map(
        shards,
        mesh=mesh,
        in_specs=(
            P("sp", "tp"),
            P("sp", "tp"),
            P("tp", None),
            P("tp", None),
            P("tp"),
            P(None, "tp", None, None),
            P(None, "tp", None, None),
            P("tp"),
            P("tp", None),
            P(("sp", "tp"), None),
            P(),
            P(("sp", "tp"), None),
            P(("sp", "tp"), None),
            P("sp", None, "tp"),
            P("sp", None, "tp"),
            P("sp", "tp", None),
        ),
        out_specs=P(("sp", "tp"), None),
        check_vma=False,
    )
```

```python
import functools

import jax
import jax.numpy as jnp
from jax import lax
from jax.experimental import pallas as pl
from jax.experimental.pallas import tpu as pltpu
from jax.sharding import PartitionSpec as P


EPS = 1e-06


LANES = 8
EXACT = lax.Precision.HIGHEST


def one_hot(shape, test):
    rows = lax.broadcasted_iota(jnp.int32, shape, 0)
    columns = lax.broadcasted_iota(jnp.int32, shape, 1)
    return jnp.where(test(rows, columns), 1.0, 0.0).astype(jnp.float32)


def exact_dot(left, right, transposed=False):
    contract = ((1,), (1,)) if transposed else ((1,), (0,))
    return lax.dot_general(
        left, right, (contract, ((), ())), precision=EXACT, preferred_element_type=jnp.float32
    )


def complex_times(a_real, a_imag, b_real, b_imag):
    return a_real * b_real - a_imag * b_imag, a_real * b_imag + a_imag * b_real


def states_kernel(
    input_hbm,
    shift_hbm,
    pole_real_hbm,
    pole_imag_hbm,
    log_step_hbm,
    map_hbm,
    total_ref,
    drive_real_ref,
    drive_imag_ref,
    scale_ref,
    factor_ref,
    enter_ref,
    input_ref,
    shift_ref,
    pole_real_ref,
    pole_imag_ref,
    log_step_ref,
    map_ref,
    semaphores,
):
    sources = (pole_real_hbm, pole_imag_hbm, log_step_hbm, shift_hbm, input_hbm, map_hbm)
    targets = (pole_real_ref, pole_imag_ref, log_step_ref, shift_ref, input_ref, map_ref)
    copies = [
        pltpu.make_async_copy(source, target, semaphores.at[number])
        for number, (source, target) in enumerate(zip(sources, targets))
    ]
    for copy in copies:
        copy.start()
    for copy in copies:
        copy.wait()
    rows = input_ref.shape[0]
    groups, states = pole_real_ref.shape
    width = groups * states
    channels = map_ref.shape[1] // groups
    length = rows // LANES
    spread = one_hot((states, width), lambda r, c: c % states == r)
    group_of = one_hot((groups, width), lambda r, c: c // states == r)

    def in_a_row(ref):
        return jnp.sum(exact_dot(ref[...], spread) * group_of, axis=0, keepdims=True)

    pole_real, pole_imag = in_a_row(pole_real_ref), in_a_row(pole_imag_ref)
    logs = jnp.broadcast_to(log_step_ref[...], (groups, groups))
    step = jnp.exp(exact_dot(logs, group_of)[:1])
    magnitude = jnp.exp(pole_real * step)
    factor_real = magnitude * jnp.cos(pole_imag * step)
    factor_imag = magnitude * jnp.sin(pole_imag * step)
    denominator = pole_real * pole_real + pole_imag * pole_imag
    ratio_real = ((factor_real - 1.0) * pole_real + factor_imag * pole_imag) / denominator
    ratio_imag = (factor_imag * pole_real - (factor_real - 1.0) * pole_imag) / denominator
    factor_ref[0:1, :] = factor_real
    factor_ref[1:2, :] = factor_imag

    order = one_hot((rows, rows), lambda r, c: c == (r % LANES) * length + r // LANES)
    inputs = jnp.dot(
        order.astype(jnp.bfloat16), input_ref[...], preferred_element_type=jnp.float32
    )
    scale_ref[...] = exact_dot(exact_dot(order, jnp.exp(shift_ref[...]), True), group_of)
    same_group = one_hot(
        (groups * channels, width), lambda r, c: r // channels == c // states
    )
    plain_real = exact_dot(inputs, exact_dot(map_ref[0], spread) * same_group)
    plain_imag = exact_dot(inputs, exact_dot(map_ref[1], spread) * same_group)
    drive_real, drive_imag = complex_times(ratio_real, ratio_imag, plain_real, plain_imag)
    drive_real_ref[...] = drive_real
    drive_imag_ref[...] = drive_imag

    wide_real = jnp.broadcast_to(factor_real, (LANES, width))
    wide_imag = jnp.broadcast_to(factor_imag, (LANES, width))
    through_real = jnp.ones((LANES, width), jnp.float32)
    through_imag = state_real = state_imag = jnp.zeros((LANES, width), jnp.float32)

    def advance(k, held):
        through_real, through_imag, state_real, state_imag = held
        at = pl.ds(pl.multiple_of(k * LANES, LANES), LANES)
        scale = scale_ref[at, :]
        real, imag = scale * wide_real, scale * wide_imag
        through_real, through_imag = complex_times(real, imag, through_real, through_imag)
        state_real, state_imag = complex_times(real, imag, state_real, state_imag)
        state_real = state_real + drive_real_ref[at, :]
        state_imag = state_imag + drive_imag_ref[at, :]
        return through_real, through_imag, state_real, state_imag

    through_real, through_imag, state_real, state_imag = lax.fori_loop(
        0, length, advance, (through_real, through_imag, state_real, state_imag), unroll=8
    )

    place = lax.broadcasted_iota(jnp.int32, (LANES, width), 0)

    def moved(value, by, empty):
        return jnp.where(place >= by, pltpu.roll(value, by, 0), empty)

    by = 1
    while by < LANES:
        a_real, a_imag = moved(through_real, by, 1.0), moved(through_imag, by, 0.0)
        x_real, x_imag = moved(state_real, by, 0.0), moved(state_imag, by, 0.0)
        x_real, x_imag = complex_times(through_real, through_imag, x_real, x_imag)
        state_real, state_imag = state_real + x_real, state_imag + x_imag
        through_real, through_imag = complex_times(through_real, through_imag, a_real, a_imag)
        by *= 2
    enter_ref[0] = moved(through_real, 1, 1.0)
    enter_ref[1] = moved(through_imag, 1, 0.0)
    enter_ref[2] = moved(state_real, 1, 0.0)
    enter_ref[3] = moved(state_imag, 1, 0.0)
    total = jnp.concatenate(
        [v[LANES - 1 :] for v in (through_real, through_imag, state_real, state_imag)], axis=0
    )
    total_ref[...] = jnp.broadcast_to(total[None], total_ref.shape)


def response_kernel(here_ref, *refs):
    sources, (out_ref, state_ref), targets, semaphores = (
        refs[:9],
        refs[9:11],
        refs[11:20],
        refs[20],
    )
    copies = [
        pltpu.make_async_copy(source, target, semaphores.at[number])
        for number, (source, target) in enumerate(zip(sources, targets))
    ]
    for copy in copies:
        copy.start()
    (
        arrived_ref,
        drive_real_ref,
        drive_imag_ref,
        scale_ref,
        factor_ref,
        enter_ref,
        input_ref,
        readout_ref,
        skip_ref,
    ) = targets
    copies[0].wait()
    rows = input_ref.shape[0]
    width = factor_ref.shape[1]
    states = readout_ref.shape[2]
    channels = readout_ref.shape[1] * states // width
    length = rows // LANES
    here = here_ref[0]
    carry_real = carry_imag = jnp.zeros((1, width), jnp.float32)
    for j in range(arrived_ref.shape[0]):
        block = arrived_ref[j]
        real, imag = complex_times(block[0:1], block[1:2], carry_real, carry_imag)
        earlier = j < here
        carry_real = jnp.where(earlier, real + block[2:3], carry_real)
        carry_imag = jnp.where(earlier, imag + block[3:4], carry_imag)
    for copy in copies[1:]:
        copy.wait()
    state_real, state_imag = complex_times(enter_ref[0], enter_ref[1], carry_real, carry_imag)
    state_real, state_imag = state_real + enter_ref[2], state_imag + enter_ref[3]
    wide_real = jnp.broadcast_to(factor_ref[0:1, :], (LANES, width))
    wide_imag = jnp.broadcast_to(factor_ref[1:2, :], (LANES, width))

    def advance(k, held):
        state_real, state_imag = held
        at = pl.ds(pl.multiple_of(k * LANES, LANES), LANES)
        scale = scale_ref[at, :]
        real, imag = scale * wide_real, scale * wide_imag
        state_real, state_imag = complex_times(real, imag, state_real, state_imag)
        state_real = state_real + drive_real_ref[at, :]
        state_imag = state_imag + drive_imag_ref[at, :]
        state_ref[at, :width] = state_real
        state_ref[at, width:] = state_imag
        return state_real, state_imag

    lax.fori_loop(0, length, advance, (state_real, state_imag), unroll=8)
    spread = one_hot((states, width), lambda r, c: c % states == r)
    same_group = one_hot(
        (readout_ref.shape[1], width), lambda r, c: r // channels == c // states
    )
    matrix = jnp.concatenate(
        [
            exact_dot(readout_ref[0], spread) * same_group,
            exact_dot(readout_ref[1], spread) * -same_group,
        ],
        axis=1,
    )
    response = exact_dot(state_ref[...], matrix, True)
    order = one_hot((rows, rows), lambda r, c: r == (c % LANES) * length + c // LANES)
    response = exact_dot(order, response) + skip_ref[...] * input_ref[...].astype(jnp.float32)
    out_ref[...] = jax.nn.gelu(response).astype(jnp.bfloat16)


def local_states(
    mixer_input, decay_shift, pole_real, pole_imaginary, log_step, input_map, devices
):
    rows = mixer_input.shape[0]
    groups, states = pole_real.shape
    width = groups * states
    f32 = jnp.float32
    shape = jax.ShapeDtypeStruct
    operands = (
        mixer_input,
        decay_shift.T,
        pole_real,
        pole_imaginary,
        log_step[None],
        jnp.swapaxes(input_map, 2, 3).reshape(2, -1, states),
    )
    return pl.pallas_call(
        states_kernel,
        out_shape=(
            shape((devices, 4, width), f32),
            shape((rows, width), f32),
            shape((rows, width), f32),
            shape((rows, width), f32),
            shape((2, width), f32),
            shape((4, LANES, width), f32),
        ),
        in_specs=[pl.BlockSpec(memory_space=pltpu.HBM)] * len(operands),
        scratch_shapes=[pltpu.VMEM(operand.shape, operand.dtype) for operand in operands]
        + [pltpu.SemaphoreType.DMA((len(operands),))],
        compiler_params=pltpu.CompilerParams(vmem_limit_bytes=60 * 1024 * 1024),
        name="states",
    )(*operands)


def activations(here, arrived, kept, mixer_input, readout_matrix, skip):
    rows, channels = mixer_input.shape
    width = arrived.shape[2]
    operands = (
        arrived,
        *kept,
        mixer_input,
        readout_matrix.reshape(2, channels, -1),
        skip[None],
    )
    return pl.pallas_call(
        response_kernel,
        out_shape=jax.ShapeDtypeStruct((rows, channels), jnp.bfloat16),
        in_specs=[pl.BlockSpec(memory_space=pltpu.SMEM)]
        + [pl.BlockSpec(memory_space=pltpu.HBM)] * len(operands),
        scratch_shapes=[pltpu.VMEM((rows, 2 * width), jnp.float32)]
        + [pltpu.VMEM(operand.shape, operand.dtype) for operand in operands]
        + [pltpu.SemaphoreType.DMA((len(operands),))],
        compiler_params=pltpu.CompilerParams(vmem_limit_bytes=60 * 1024 * 1024),
        name="response",
    )(here.reshape(1), *operands)


def experts_kernel(capacity, count, sets, *refs):
    row_refs, refs = refs[:count], refs[count:]
    weights, outs = refs[: 3 * sets], refs[3 * sets :]
    held, part = row_refs[0].shape[0] // 2, row_refs[0].shape[1]

    def whole_rows(half):
        return one_hot(
            (held, 2 * held),
            lambda r, c: c == r // capacity * (2 * capacity) + r % capacity + half * capacity,
        ).astype(jnp.bfloat16)

    pick = [whole_rows(half) for half in range(2)]
    pieces = [
        jnp.concatenate(
            [jnp.dot(chosen, ref[...], preferred_element_type=jnp.float32) for ref in row_refs],
            axis=0,
        ).astype(jnp.bfloat16)
        for chosen in pick
    ]
    total = None
    for number in range(sets):
        gate_ref, up_ref, down_ref = weights[3 * number : 3 * number + 3]

        def product(ref):
            return sum(
                jnp.dot(
                    piece,
                    ref[half * part : (half + 1) * part, :],
                    preferred_element_type=jnp.float32,
                )
                for half, piece in enumerate(pieces)
            )

        hidden = (jax.nn.silu(product(gate_ref)) * product(up_ref)).astype(jnp.bfloat16)
        out = jnp.dot(hidden, down_ref[...], preferred_element_type=jnp.float32)
        total = out if total is None else total + out
    total = total.astype(jnp.bfloat16)
    for number, ref in enumerate(outs):
        rows = total[number * held : (number + 1) * held]
        ref[...] = sum(
            lax.dot_general(
                pick[half],
                rows[:, half * part : (half + 1) * part],
                (((0,), (0,)), ((), ())),
                preferred_element_type=jnp.float32,
            )
            for half in range(2)
        ).astype(jnp.bfloat16)


def partial_out(rows, weights, capacity):
    count, sets = len(rows), len(weights) // 3
    out = jax.ShapeDtypeStruct(rows[0].shape, jnp.bfloat16)
    flops = count * rows[0].shape[0] * sum(w.size for w in weights)
    return pl.pallas_call(
        functools.partial(experts_kernel, capacity, count, sets),
        out_shape=(out,) * count,
        in_specs=[pl.BlockSpec(memory_space=pltpu.VMEM)] * (count + len(weights)),
        compiler_params=pltpu.CompilerParams(vmem_limit_bytes=12 << 20),
        cost_estimate=pl.CostEstimate(flops=flops, bytes_accessed=0, transcendentals=0),
        name="experts",
    )(*rows, *weights)


def stage_kernel(*refs):
    count = len(refs) // 2
    copies = [
        pltpu.make_async_copy(refs[number], refs[count + number], refs[-1].at[number])
        for number in range(count)
    ]
    for copy in copies:
        copy.start()
    for copy in copies:
        copy.wait()


def staged(arrays):
    return pl.pallas_call(
        stage_kernel,
        out_shape=[jax.ShapeDtypeStruct(array.shape, array.dtype) for array in arrays],
        in_specs=[pl.BlockSpec(memory_space=pltpu.HBM)] * len(arrays),
        out_specs=[pl.BlockSpec(memory_space=pltpu.VMEM)] * len(arrays),
        scratch_shapes=[pltpu.SemaphoreType.DMA((len(arrays),))],
        compiler_params=pltpu.CompilerParams(vmem_limit_bytes=32 << 20),
        cost_estimate=pl.CostEstimate(flops=1 << 33, bytes_accessed=0, transcendentals=0),
        name="stage",
    )(*arrays)


def slot_numbers(route_rows, experts, capacity):
    flat = route_rows.reshape(route_rows.shape[:-2] + (-1,))
    matches = (flat[..., None] == jnp.arange(experts, dtype=jnp.int32)).astype(jnp.int32)
    earlier = jnp.cumsum(matches, axis=-2) - matches
    return flat * capacity + jnp.sum(earlier * matches, axis=-1)


def half_places(slots, capacity):
    first = slots // capacity * (2 * capacity) + slots % capacity
    return jnp.stack([first, first + capacity])


def chip_shift(distance, flip=0):
    size = lax.axis_size("tp")
    chips = size // 2
    return [
        (2 * chip + core, 2 * ((chip + distance) % chips) + (core ^ flip))
        for chip in range(chips)
        for core in range(2)
    ]


def gathered_projection(out_proj):
    chips = lax.axis_size("tp") // 2
    mine = [out_proj] + [
        lax.ppermute(out_proj, "tp", chip_shift(distance)) for distance in range(1, chips)
    ]
    other = [lax.ppermute(block, "tp", chip_shift(0, 1)) for block in mine]
    return (*mine, *other)


def mix_kernel(order_ref, arrived_ref, stream_ref, gain_ref, places_ref, *refs):
    *blocks, mixed_ref, outgoing_ref = refs
    tokens, model = stream_ref.shape
    projected = sum(
        jnp.dot(arrived_ref[order_ref[number]], block[...], preferred_element_type=jnp.float32)
        for number, block in enumerate(blocks)
    )
    mixed = (stream_ref[...].astype(jnp.float32) + projected).astype(jnp.bfloat16)
    mixed_ref[...] = mixed
    wide = mixed.astype(jnp.float32)
    mean = jnp.mean(wide * wide, axis=-1, keepdims=True)
    normed = (wide * lax.rsqrt(mean + EPS) * gain_ref[...]).astype(jnp.bfloat16)
    halves = jnp.concatenate([normed[:, : model // 2], normed[:, model // 2 :]], axis=0)
    width = outgoing_ref.shape[0]
    at = lax.broadcasted_iota(jnp.int32, (2 * tokens, width), 1)
    hits = sum(
        jnp.where(at == places_ref[:, k : k + 1], 1.0, 0.0) for k in range(places_ref.shape[1])
    ).astype(jnp.bfloat16)
    outgoing_ref[...] = lax.dot_general(
        hits, halves, (((0,), (0,)), ((), ())), preferred_element_type=jnp.float32
    ).astype(jnp.bfloat16)


def mixed_and_outgoing(activated, blocks, stream, norm_gain, places, width):
    size = lax.axis_size("tp")
    chips = size // 2
    here = lax.axis_index("tp")
    chip, core = here // 2, here % 2
    tokens, model = stream.shape
    back = 2 * ((chip - jnp.arange(chips, dtype=jnp.int32)) % chips)
    order = jnp.concatenate([back + core, back + 1 - core])
    arrived = lax.all_to_all(
        activated.reshape(size, tokens, -1), "tp", split_axis=0, concat_axis=0, tiled=True
    )
    vmem = pl.BlockSpec(memory_space=pltpu.VMEM)
    shape = jax.ShapeDtypeStruct
    return pl.pallas_call(
        mix_kernel,
        out_shape=(
            shape((tokens, model), jnp.bfloat16),
            shape((width, model // 2), jnp.bfloat16),
        ),
        in_specs=[pl.BlockSpec(memory_space=pltpu.SMEM)]
        + [vmem] * (4 + size),
        compiler_params=pltpu.CompilerParams(vmem_limit_bytes=12 << 20),
        name="mix",
    )(order, arrived, stream, norm_gain[None], places.reshape(2 * tokens, -1), *blocks)


def over_experts(halves, experts):
    blocks = halves.reshape(experts, -1, halves.shape[1])
    return lax.all_to_all(blocks, "sp", split_axis=0, concat_axis=0, tiled=True).reshape(
        halves.shape
    )


def expert_over_chips(rows, w_gate, w_up, w_down, w_up_other, w_down_other, capacity):
    rows, sent, *kept = lax.optimization_barrier(
        (rows, w_gate, w_gate, w_up, w_down, w_up_other, w_down_other)
    )
    before = lax.ppermute(rows, "tp", chip_shift(1))
    after = lax.ppermute(rows, "tp", chip_shift(-1))
    w_gate_other = lax.ppermute(sent, "tp", chip_shift(0, 1))
    w_gate, w_up, w_down, w_up_other, w_down_other = staged(kept)
    weights = (w_gate, w_up, w_down, w_gate_other, w_up_other, w_down_other)
    before, after, *weights = lax.optimization_barrier((before, after, *weights))
    middle = rows.shape[0] // 2
    across = (
        lax.ppermute(before[:middle], "tp", chip_shift(1)),
        lax.ppermute(after[middle:], "tp", chip_shift(-1)),
    )
    (for_before,) = partial_out((before,), weights, capacity)
    to_before = lax.ppermute(for_before, "tp", chip_shift(-1))
    after, for_before = lax.optimization_barrier((after, for_before))
    (for_after,) = partial_out((after,), weights, capacity)
    to_after = lax.ppermute(for_after, "tp", chip_shift(1))
    across, for_after = lax.optimization_barrier((across, for_after))
    for_across = partial_out(across, weights, capacity)
    to_across = [lax.ppermute(part, "tp", chip_shift(2)) for part in for_across]
    rows, _ = lax.optimization_barrier((rows, for_across))
    (total,) = partial_out((rows,), weights, capacity)
    total = total.astype(jnp.float32) + to_before.astype(jnp.float32)
    total = lax.optimization_barrier(total + to_after.astype(jnp.float32))
    total = total + jnp.concatenate(to_across, axis=0).astype(jnp.float32)
    return total.astype(jnp.bfloat16)


def spread_weights(places, weights, width):
    tokens, top = weights.shape
    hits = places.reshape(2, tokens, top)[..., None] == jnp.arange(width, dtype=jnp.int32)
    spread = jnp.sum(jnp.where(hits, weights[None, :, :, None], 0.0), axis=2)
    spread = spread.reshape(2 * tokens, width)
    high = spread.astype(jnp.bfloat16)
    return jnp.concatenate([high, (spread - high.astype(jnp.float32)).astype(jnp.bfloat16)])


def weighted_pick(spread, returned_result):
    parts = jnp.dot(spread, returned_result, preferred_element_type=jnp.float32)
    return parts[: len(parts) // 2] + parts[len(parts) // 2 :]


def shards(
    mixer_input,
    decay_shift,
    pole_real,
    pole_imaginary,
    log_step,
    input_map,
    readout_matrix,
    skip,
    out_proj,
    stream,
    norm_gain,
    routes,
    route_logits,
    w_gate,
    w_up,
    w_down,
):
    w_down_other = lax.ppermute(w_down[0], "tp", chip_shift(0, 1))
    w_up_other = lax.ppermute(w_up[0], "tp", chip_shift(0, 1))
    totals, *kept = local_states(
        mixer_input,
        decay_shift,
        pole_real,
        pole_imaginary,
        log_step,
        input_map,
        lax.axis_size("sp"),
    )
    ends = lax.all_to_all(totals, "sp", split_axis=0, concat_axis=0, tiled=True)
    blocks = gathered_projection(out_proj)
    own_rows, _ = stream.shape
    weights = jax.nn.sigmoid(
        jnp.stack(
            [route_logits[:, 0] - route_logits[:, 1], route_logits[:, 1] - route_logits[:, 0]],
            axis=1,
        )
    )
    experts = lax.axis_size("sp") * w_gate.shape[0]
    capacity = 4 * own_rows // experts
    width = 2 * experts * capacity
    places = half_places(slot_numbers(routes, experts, capacity), capacity)
    spread = spread_weights(places, weights, width)
    ends, spread, places = lax.optimization_barrier((ends, spread, places))
    activated = activations(
        lax.axis_index("sp"), ends, kept, mixer_input, readout_matrix, skip
    )
    mixed, outgoing = mixed_and_outgoing(
        activated, blocks, stream, norm_gain, places, width
    )
    mixed_wide = mixed.astype(jnp.float32)

    arrived = over_experts(outgoing, experts)
    summed = expert_over_chips(
        arrived, w_gate[0], w_up[0], w_down[0], w_up_other, w_down_other, capacity
    )
    picked = weighted_pick(spread, over_experts(summed, experts))
    picked = jnp.concatenate([picked[:own_rows], picked[own_rows:]], axis=1)
    return (mixed_wide + picked).astype(jnp.bfloat16)


def solution(mesh):
    return jax.shard_map(
        shards,
        mesh=mesh,
        in_specs=(
            P("sp", "tp"),
            P("sp", "tp"),
            P("tp", None),
            P("tp", None),
            P("tp"),
            P(None, "tp", None, None),
            P(None, "tp", None, None),
            P("tp"),
            P("tp", None),
            P(("sp", "tp"), None),
            P(),
            P(("sp", "tp"), None),
            P(("sp", "tp"), None),
            P("sp", None, "tp"),
            P("sp", None, "tp"),
            P("sp", "tp", None),
        ),
        out_specs=P(("sp", "tp"), None),
        check_vma=False,
    )
```

```python
import functools

import jax
import jax.numpy as jnp
from jax import lax
from jax.experimental import pallas as pl
from jax.experimental.pallas import tpu as pltpu
from jax.sharding import PartitionSpec as P


EPS = 1e-06


LANES = 8
EXACT = lax.Precision.HIGHEST


def one_hot(shape, test):
    rows = lax.broadcasted_iota(jnp.int32, shape, 0)
    columns = lax.broadcasted_iota(jnp.int32, shape, 1)
    return jnp.where(test(rows, columns), 1.0, 0.0).astype(jnp.float32)


def exact_dot(left, right, transposed=False):
    contract = ((1,), (1,)) if transposed else ((1,), (0,))
    return lax.dot_general(
        left, right, (contract, ((), ())), precision=EXACT, preferred_element_type=jnp.float32
    )


def whole_dot(left, right, transposed=False):
    contract = (((1,), (1 if transposed else 0,)), ((), ()))
    plain = left if left.dtype == jnp.bfloat16 else right
    rest = right if left.dtype == jnp.bfloat16 else left
    total = None
    for _ in range(3):
        part = rest.astype(jnp.bfloat16)
        rest = rest - part.astype(jnp.float32)
        pair = (plain, part) if plain is left else (part, plain)
        term = lax.dot_general(*pair, contract, preferred_element_type=jnp.float32)
        total = term if total is None else total + term
    return total


def complex_times(a_real, a_imag, b_real, b_imag):
    return a_real * b_real - a_imag * b_imag, a_real * b_imag + a_imag * b_real


def states_kernel(
    input_hbm,
    shift_hbm,
    pole_real_hbm,
    pole_imag_hbm,
    log_step_hbm,
    map_hbm,
    total_ref,
    drive_real_ref,
    drive_imag_ref,
    scale_ref,
    factor_ref,
    enter_ref,
    input_ref,
    shift_ref,
    pole_real_ref,
    pole_imag_ref,
    log_step_ref,
    map_ref,
    semaphores,
):
    sources = (pole_real_hbm, pole_imag_hbm, log_step_hbm, shift_hbm, input_hbm, map_hbm)
    targets = (pole_real_ref, pole_imag_ref, log_step_ref, shift_ref, input_ref, map_ref)
    copies = [
        pltpu.make_async_copy(source, target, semaphores.at[number])
        for number, (source, target) in enumerate(zip(sources, targets))
    ]
    for copy in copies:
        copy.start()
    for copy in copies:
        copy.wait()
    rows = input_ref.shape[0]
    groups, states = pole_real_ref.shape
    width = groups * states
    channels = map_ref.shape[1] // groups
    length = rows // LANES
    spread = one_hot((states, width), lambda r, c: c % states == r).astype(jnp.bfloat16)
    group_of = one_hot((groups, width), lambda r, c: c // states == r)

    def in_a_row(ref):
        return jnp.sum(whole_dot(ref[...], spread) * group_of, axis=0, keepdims=True)

    pole_real, pole_imag = in_a_row(pole_real_ref), in_a_row(pole_imag_ref)
    logs = jnp.broadcast_to(log_step_ref[...], (groups, groups))
    step = jnp.exp(whole_dot(logs, group_of.astype(jnp.bfloat16))[:1])
    magnitude = jnp.exp(pole_real * step)
    factor_real = magnitude * jnp.cos(pole_imag * step)
    factor_imag = magnitude * jnp.sin(pole_imag * step)
    denominator = pole_real * pole_real + pole_imag * pole_imag
    ratio_real = ((factor_real - 1.0) * pole_real + factor_imag * pole_imag) / denominator
    ratio_imag = (factor_imag * pole_real - (factor_real - 1.0) * pole_imag) / denominator
    factor_ref[0:1, :] = factor_real
    factor_ref[1:2, :] = factor_imag

    order = one_hot((rows, rows), lambda r, c: c == (r % LANES) * length + r // LANES)
    order = order.astype(jnp.bfloat16)
    inputs = jnp.dot(order, input_ref[...], preferred_element_type=jnp.float32)
    inputs = inputs.astype(jnp.bfloat16)
    scale_ref[...] = whole_dot(
        whole_dot(order, jnp.exp(shift_ref[...]), True), group_of.astype(jnp.bfloat16)
    )
    same_group = one_hot(
        (groups * channels, width), lambda r, c: r // channels == c // states
    )
    plain_real = whole_dot(inputs, whole_dot(map_ref[0], spread) * same_group)
    plain_imag = whole_dot(inputs, whole_dot(map_ref[1], spread) * same_group)
    drive_real, drive_imag = complex_times(ratio_real, ratio_imag, plain_real, plain_imag)
    drive_real_ref[...] = drive_real
    drive_imag_ref[...] = drive_imag

    wide_real = jnp.broadcast_to(factor_real, (LANES, width))
    wide_imag = jnp.broadcast_to(factor_imag, (LANES, width))
    through_real = jnp.ones((LANES, width), jnp.float32)
    through_imag = state_real = state_imag = jnp.zeros((LANES, width), jnp.float32)

    def advance(k, held):
        through_real, through_imag, state_real, state_imag = held
        at = pl.ds(pl.multiple_of(k * LANES, LANES), LANES)
        scale = scale_ref[at, :]
        real, imag = scale * wide_real, scale * wide_imag
        through_real, through_imag = complex_times(real, imag, through_real, through_imag)
        state_real, state_imag = complex_times(real, imag, state_real, state_imag)
        state_real = state_real + drive_real_ref[at, :]
        state_imag = state_imag + drive_imag_ref[at, :]
        return through_real, through_imag, state_real, state_imag

    through_real, through_imag, state_real, state_imag = lax.fori_loop(
        0, length, advance, (through_real, through_imag, state_real, state_imag), unroll=4
    )

    place = lax.broadcasted_iota(jnp.int32, (LANES, width), 0)

    def moved(value, by, empty):
        return jnp.where(place >= by, pltpu.roll(value, by, 0), empty)

    by = 1
    while by < LANES:
        a_real, a_imag = moved(through_real, by, 1.0), moved(through_imag, by, 0.0)
        x_real, x_imag = moved(state_real, by, 0.0), moved(state_imag, by, 0.0)
        x_real, x_imag = complex_times(through_real, through_imag, x_real, x_imag)
        state_real, state_imag = state_real + x_real, state_imag + x_imag
        through_real, through_imag = complex_times(through_real, through_imag, a_real, a_imag)
        by *= 2
    enter_ref[0] = moved(through_real, 1, 1.0)
    enter_ref[1] = moved(through_imag, 1, 0.0)
    enter_ref[2] = moved(state_real, 1, 0.0)
    enter_ref[3] = moved(state_imag, 1, 0.0)
    total = jnp.concatenate(
        [v[LANES - 1 :] for v in (through_real, through_imag, state_real, state_imag)], axis=0
    )
    total_ref[...] = jnp.broadcast_to(total[None], total_ref.shape)


def alone_kernel(
    drive_real_ref,
    drive_imag_ref,
    scale_ref,
    factor_ref,
    enter_ref,
    input_ref,
    readout_ref,
    skip_ref,
    alone_ref,
    through_ref,
    matrix_ref,
    state_ref,
    product_ref,
):
    rows = input_ref.shape[0]
    width = factor_ref.shape[1]
    states = readout_ref.shape[2]
    channels = readout_ref.shape[1] * states // width
    length = rows // LANES
    wide_real = jnp.broadcast_to(factor_ref[0:1, :], (LANES, width))
    wide_imag = jnp.broadcast_to(factor_ref[1:2, :], (LANES, width))

    def advance(k, held):
        through_real, through_imag, state_real, state_imag = held
        at = pl.ds(pl.multiple_of(k * LANES, LANES), LANES)
        scale = scale_ref[at, :]
        real, imag = scale * wide_real, scale * wide_imag
        through_real, through_imag = complex_times(real, imag, through_real, through_imag)
        state_real, state_imag = complex_times(real, imag, state_real, state_imag)
        state_real = state_real + drive_real_ref[at, :]
        state_imag = state_imag + drive_imag_ref[at, :]
        product_ref[at, :width] = through_real
        product_ref[at, width:] = through_imag
        state_ref[at, :width] = state_real
        state_ref[at, width:] = state_imag
        return through_real, through_imag, state_real, state_imag

    lax.fori_loop(0, length, advance, tuple(enter_ref[i] for i in range(4)), unroll=4)
    spread = one_hot((states, width), lambda r, c: c % states == r).astype(jnp.bfloat16)
    same_group = one_hot(
        (readout_ref.shape[1], width), lambda r, c: r // channels == c // states
    )
    matrix_ref[:, :width] = whole_dot(readout_ref[0], spread) * same_group
    matrix_ref[:, width:] = whole_dot(readout_ref[1], spread) * -same_group
    response = exact_dot(state_ref[...], matrix_ref[...], True)
    order = one_hot((rows, rows), lambda r, c: r == (c % LANES) * length + c // LANES)
    alone_ref[...] = whole_dot(order.astype(jnp.bfloat16), response) + skip_ref[...] * input_ref[...].astype(
        jnp.float32
    )
    through_ref[...] = whole_dot(order.astype(jnp.bfloat16), product_ref[...])


def response_kernel(here_ref, arrived_ref, alone_ref, through_ref, matrix_ref, out_ref):
    width = arrived_ref.shape[2]
    here = here_ref[0]

    def pass_on(j, carry):
        block = arrived_ref[j]
        real, imag = complex_times(block[0:1], block[1:2], *carry)
        earlier = j < here
        return (
            jnp.where(earlier, real + block[2:3], carry[0]),
            jnp.where(earlier, imag + block[3:4], carry[1]),
        )

    zero = jnp.zeros((1, width), jnp.float32)
    carry = lax.fori_loop(0, arrived_ref.shape[0], pass_on, (zero, zero), unroll=8)
    extra = jnp.concatenate(
        complex_times(through_ref[:, :width], through_ref[:, width:], *carry), axis=1
    )
    response = alone_ref[...] + exact_dot(extra, matrix_ref[...], True)
    out_ref[...] = jax.nn.gelu(response).astype(jnp.bfloat16)


def local_states(
    mixer_input, decay_shift, pole_real, pole_imaginary, log_step, input_map, devices
):
    rows = mixer_input.shape[0]
    groups, states = pole_real.shape
    width = groups * states
    f32 = jnp.float32
    shape = jax.ShapeDtypeStruct
    operands = (
        mixer_input,
        decay_shift.T,
        pole_real,
        pole_imaginary,
        log_step[None],
        jnp.swapaxes(input_map, 2, 3).reshape(2, -1, states),
    )
    return pl.pallas_call(
        states_kernel,
        out_shape=(
            shape((devices, 4, width), f32),
            shape((rows, width), f32),
            shape((rows, width), f32),
            shape((rows, width), f32),
            shape((2, width), f32),
            shape((4, LANES, width), f32),
        ),
        in_specs=[pl.BlockSpec(memory_space=pltpu.HBM)] * len(operands),
        scratch_shapes=[pltpu.VMEM(operand.shape, operand.dtype) for operand in operands]
        + [pltpu.SemaphoreType.DMA((len(operands),))],
        compiler_params=pltpu.CompilerParams(vmem_limit_bytes=60 * 1024 * 1024),
        name="states",
    )(*operands)


def response_alone(kept, mixer_input, readout_matrix, skip):
    rows, channels = mixer_input.shape
    width = kept[0].shape[1]
    shape = jax.ShapeDtypeStruct
    wide = pltpu.VMEM((rows, 2 * width), jnp.float32)
    return pl.pallas_call(
        alone_kernel,
        out_shape=(
            shape((rows, channels), jnp.float32),
            shape((rows, 2 * width), jnp.float32),
            shape((channels, 2 * width), jnp.float32),
        ),
        scratch_shapes=[wide, wide],
        compiler_params=pltpu.CompilerParams(vmem_limit_bytes=16 << 20),
        name="alone",
    )(*kept, mixer_input, readout_matrix.reshape(2, channels, -1), skip[None])


def activations(here, arrived, alone):
    vmem = pl.BlockSpec(memory_space=pltpu.VMEM)
    return pl.pallas_call(
        response_kernel,
        out_shape=jax.ShapeDtypeStruct(alone[0].shape, jnp.bfloat16),
        in_specs=[pl.BlockSpec(memory_space=pltpu.SMEM)] + [vmem] * 4,
        compiler_params=pltpu.CompilerParams(vmem_limit_bytes=16 << 20),
        name="response",
    )(here.reshape(1), arrived, *alone)


def experts_kernel(capacity, count, sets, *refs):
    row_refs, refs = refs[:count], refs[count:]
    weights, outs = refs[: 3 * sets], refs[3 * sets :]
    held, part = row_refs[0].shape[0] // 2, row_refs[0].shape[1]

    def whole_rows(half):
        return one_hot(
            (held, 2 * held),
            lambda r, c: c == r // capacity * (2 * capacity) + r % capacity + half * capacity,
        ).astype(jnp.bfloat16)

    pick = [whole_rows(half) for half in range(2)]
    pieces = [
        jnp.concatenate(
            [jnp.dot(chosen, ref[...], preferred_element_type=jnp.float32) for ref in row_refs],
            axis=0,
        ).astype(jnp.bfloat16)
        for chosen in pick
    ]
    total = None
    for number in range(sets):
        gate_ref, up_ref, down_ref = weights[3 * number : 3 * number + 3]

        def product(ref):
            return sum(
                jnp.dot(
                    piece,
                    ref[half * part : (half + 1) * part, :],
                    preferred_element_type=jnp.float32,
                )
                for half, piece in enumerate(pieces)
            )

        hidden = (jax.nn.silu(product(gate_ref)) * product(up_ref)).astype(jnp.bfloat16)
        out = jnp.dot(hidden, down_ref[...], preferred_element_type=jnp.float32)
        total = out if total is None else total + out
    total = total.astype(jnp.bfloat16)
    for number, ref in enumerate(outs):
        rows = total[number * held : (number + 1) * held]
        ref[...] = sum(
            lax.dot_general(
                pick[half],
                rows[:, half * part : (half + 1) * part],
                (((0,), (0,)), ((), ())),
                preferred_element_type=jnp.float32,
            )
            for half in range(2)
        ).astype(jnp.bfloat16)


def partial_out(rows, weights, capacity):
    count, sets = len(rows), len(weights) // 3
    out = jax.ShapeDtypeStruct(rows[0].shape, jnp.bfloat16)
    flops = count * rows[0].shape[0] * sum(w.size for w in weights)
    return pl.pallas_call(
        functools.partial(experts_kernel, capacity, count, sets),
        out_shape=(out,) * count,
        in_specs=[pl.BlockSpec(memory_space=pltpu.VMEM)] * (count + len(weights)),
        compiler_params=pltpu.CompilerParams(vmem_limit_bytes=12 << 20),
        cost_estimate=pl.CostEstimate(flops=flops, bytes_accessed=0, transcendentals=0),
        name="experts",
    )(*rows, *weights)


def stage_kernel(*refs):
    count = len(refs) // 2
    copies = [
        pltpu.make_async_copy(refs[number], refs[count + number], refs[-1].at[number])
        for number in range(count)
    ]
    for copy in copies:
        copy.start()
    for copy in copies:
        copy.wait()


def staged(arrays):
    return pl.pallas_call(
        stage_kernel,
        out_shape=[jax.ShapeDtypeStruct(array.shape, array.dtype) for array in arrays],
        in_specs=[pl.BlockSpec(memory_space=pltpu.HBM)] * len(arrays),
        out_specs=[pl.BlockSpec(memory_space=pltpu.VMEM)] * len(arrays),
        scratch_shapes=[pltpu.SemaphoreType.DMA((len(arrays),))],
        compiler_params=pltpu.CompilerParams(vmem_limit_bytes=32 << 20),
        cost_estimate=pl.CostEstimate(flops=1 << 33, bytes_accessed=0, transcendentals=0),
        name="stage",
    )(*arrays)


def slot_numbers(route_rows, experts, capacity):
    flat = route_rows.reshape(route_rows.shape[:-2] + (-1,))
    matches = (flat[..., None] == jnp.arange(experts, dtype=jnp.int32)).astype(jnp.int32)
    earlier = jnp.cumsum(matches, axis=-2) - matches
    return flat * capacity + jnp.sum(earlier * matches, axis=-1)


def half_places(slots, capacity):
    first = slots // capacity * (2 * capacity) + slots % capacity
    return jnp.stack([first, first + capacity])


def chip_shift(distance, flip=0):
    size = lax.axis_size("tp")
    chips = size // 2
    return [
        (2 * chip + core, 2 * ((chip + distance) % chips) + (core ^ flip))
        for chip in range(chips)
        for core in range(2)
    ]


def gathered_projection(out_proj):
    chips = lax.axis_size("tp") // 2
    mine = [out_proj] + [
        lax.ppermute(out_proj, "tp", chip_shift(distance)) for distance in range(1, chips)
    ]
    other = [lax.ppermute(block, "tp", chip_shift(0, 1)) for block in mine]
    return (*mine, *other)


def mix_kernel(order_ref, arrived_ref, stream_ref, gain_ref, places_ref, *refs):
    *blocks, mixed_ref, outgoing_ref = refs
    tokens, model = stream_ref.shape
    projected = sum(
        jnp.dot(arrived_ref[order_ref[number]], block[...], preferred_element_type=jnp.float32)
        for number, block in enumerate(blocks)
    )
    mixed = (stream_ref[...].astype(jnp.float32) + projected).astype(jnp.bfloat16)
    mixed_ref[...] = mixed
    wide = mixed.astype(jnp.float32)
    mean = jnp.mean(wide * wide, axis=-1, keepdims=True)
    normed = (wide * lax.rsqrt(mean + EPS) * gain_ref[...]).astype(jnp.bfloat16)
    halves = jnp.concatenate([normed[:, : model // 2], normed[:, model // 2 :]], axis=0)
    width = outgoing_ref.shape[0]
    at = lax.broadcasted_iota(jnp.int32, (2 * tokens, width), 1)
    hits = sum(
        jnp.where(at == places_ref[:, k : k + 1], 1.0, 0.0) for k in range(places_ref.shape[1])
    ).astype(jnp.bfloat16)
    outgoing_ref[...] = lax.dot_general(
        hits, halves, (((0,), (0,)), ((), ())), preferred_element_type=jnp.float32
    ).astype(jnp.bfloat16)


def mixed_and_outgoing(activated, blocks, stream, norm_gain, places, width):
    size = lax.axis_size("tp")
    chips = size // 2
    here = lax.axis_index("tp")
    chip, core = here // 2, here % 2
    tokens, model = stream.shape
    back = 2 * ((chip - jnp.arange(chips, dtype=jnp.int32)) % chips)
    order = jnp.concatenate([back + core, back + 1 - core])
    arrived = lax.all_to_all(
        activated.reshape(size, tokens, -1), "tp", split_axis=0, concat_axis=0, tiled=True
    )
    vmem = pl.BlockSpec(memory_space=pltpu.VMEM)
    shape = jax.ShapeDtypeStruct
    return pl.pallas_call(
        mix_kernel,
        out_shape=(
            shape((tokens, model), jnp.bfloat16),
            shape((width, model // 2), jnp.bfloat16),
        ),
        in_specs=[pl.BlockSpec(memory_space=pltpu.SMEM)]
        + [vmem] * (4 + size),
        compiler_params=pltpu.CompilerParams(vmem_limit_bytes=12 << 20),
        name="mix",
    )(order, arrived, stream, norm_gain[None], places.reshape(2 * tokens, -1), *blocks)


def over_experts(halves, experts):
    blocks = halves.reshape(experts, -1, halves.shape[1])
    return lax.all_to_all(blocks, "sp", split_axis=0, concat_axis=0, tiled=True).reshape(
        halves.shape
    )


def expert_over_chips(rows, w_gate, w_up, w_down, w_up_other, w_down_other, capacity):
    rows, sent, *kept = lax.optimization_barrier(
        (rows, w_gate, w_gate, w_up, w_down, w_up_other, w_down_other)
    )
    before = lax.ppermute(rows, "tp", chip_shift(1))
    after = lax.ppermute(rows, "tp", chip_shift(-1))
    w_gate_other = lax.ppermute(sent, "tp", chip_shift(0, 1))
    w_gate, w_up, w_down, w_up_other, w_down_other = staged(kept)
    weights = (w_gate, w_up, w_down, w_gate_other, w_up_other, w_down_other)
    before, after, *weights = lax.optimization_barrier((before, after, *weights))
    middle = rows.shape[0] // 2
    across = (
        lax.ppermute(before[:middle], "tp", chip_shift(1)),
        lax.ppermute(after[middle:], "tp", chip_shift(-1)),
    )
    (for_before,) = partial_out((before,), weights, capacity)
    to_before = lax.ppermute(for_before, "tp", chip_shift(-1))
    after, for_before = lax.optimization_barrier((after, for_before))
    (for_after,) = partial_out((after,), weights, capacity)
    to_after = lax.ppermute(for_after, "tp", chip_shift(1))
    across, for_after = lax.optimization_barrier((across, for_after))
    for_across = partial_out(across, weights, capacity)
    to_across = [lax.ppermute(part, "tp", chip_shift(2)) for part in for_across]
    rows, _ = lax.optimization_barrier((rows, for_across))
    (total,) = partial_out((rows,), weights, capacity)
    total = total.astype(jnp.float32) + to_before.astype(jnp.float32)
    total = lax.optimization_barrier(total + to_after.astype(jnp.float32))
    total = total + jnp.concatenate(to_across, axis=0).astype(jnp.float32)
    return total.astype(jnp.bfloat16)


def spread_weights(places, weights, width):
    tokens, top = weights.shape
    hits = places.reshape(2, tokens, top)[..., None] == jnp.arange(width, dtype=jnp.int32)
    spread = jnp.sum(jnp.where(hits, weights[None, :, :, None], 0.0), axis=2)
    spread = spread.reshape(2 * tokens, width)
    high = spread.astype(jnp.bfloat16)
    return jnp.concatenate([high, (spread - high.astype(jnp.float32)).astype(jnp.bfloat16)])


def weighted_pick(spread, returned_result):
    parts = jnp.dot(spread, returned_result, preferred_element_type=jnp.float32)
    return parts[: len(parts) // 2] + parts[len(parts) // 2 :]


def shards(
    mixer_input,
    decay_shift,
    pole_real,
    pole_imaginary,
    log_step,
    input_map,
    readout_matrix,
    skip,
    out_proj,
    stream,
    norm_gain,
    routes,
    route_logits,
    w_gate,
    w_up,
    w_down,
):
    w_down_other = lax.ppermute(w_down[0], "tp", chip_shift(0, 1))
    w_up_other = lax.ppermute(w_up[0], "tp", chip_shift(0, 1))
    totals, *kept = local_states(
        mixer_input,
        decay_shift,
        pole_real,
        pole_imaginary,
        log_step,
        input_map,
        lax.axis_size("sp"),
    )
    ends = lax.all_to_all(totals, "sp", split_axis=0, concat_axis=0, tiled=True)
    blocks = gathered_projection(out_proj)
    own_rows, _ = stream.shape
    weights = jax.nn.sigmoid(
        jnp.stack(
            [route_logits[:, 0] - route_logits[:, 1], route_logits[:, 1] - route_logits[:, 0]],
            axis=1,
        )
    )
    experts = lax.axis_size("sp") * w_gate.shape[0]
    capacity = 4 * own_rows // experts
    width = 2 * experts * capacity
    places = half_places(slot_numbers(routes, experts, capacity), capacity)
    spread = spread_weights(places, weights, width)
    alone = response_alone(kept, mixer_input, readout_matrix, skip)
    ends, spread, places, *alone = lax.optimization_barrier((ends, spread, places, *alone))
    activated = activations(lax.axis_index("sp"), ends, alone)
    mixed, outgoing = mixed_and_outgoing(
        activated, blocks, stream, norm_gain, places, width
    )
    mixed_wide = mixed.astype(jnp.float32)

    arrived = over_experts(outgoing, experts)
    summed = expert_over_chips(
        arrived, w_gate[0], w_up[0], w_down[0], w_up_other, w_down_other, capacity
    )
    picked = weighted_pick(spread, over_experts(summed, experts))
    picked = jnp.concatenate([picked[:own_rows], picked[own_rows:]], axis=1)
    return (mixed_wide + picked).astype(jnp.bfloat16)


def solution(mesh):
    return jax.shard_map(
        shards,
        mesh=mesh,
        in_specs=(
            P("sp", "tp"),
            P("sp", "tp"),
            P("tp", None),
            P("tp", None),
            P("tp"),
            P(None, "tp", None, None),
            P(None, "tp", None, None),
            P("tp"),
            P("tp", None),
            P(("sp", "tp"), None),
            P(),
            P(("sp", "tp"), None),
            P(("sp", "tp"), None),
            P("sp", None, "tp"),
            P("sp", None, "tp"),
            P("sp", "tp", None),
        ),
        out_specs=P(("sp", "tp"), None),
        check_vma=False,
    )
```

```python
import functools

import jax
import jax.numpy as jnp
from jax import lax
from jax.experimental import pallas as pl
from jax.experimental.pallas import tpu as pltpu
from jax.sharding import PartitionSpec as P


EPS = 1e-06


LANES = 8
EXACT = lax.Precision.HIGHEST


def one_hot(shape, test):
    rows = lax.broadcasted_iota(jnp.int32, shape, 0)
    columns = lax.broadcasted_iota(jnp.int32, shape, 1)
    return jnp.where(test(rows, columns), 1.0, 0.0).astype(jnp.float32)


def exact_dot(left, right, transposed=False):
    contract = ((1,), (1,)) if transposed else ((1,), (0,))
    return lax.dot_general(
        left, right, (contract, ((), ())), precision=EXACT, preferred_element_type=jnp.float32
    )


def whole_dot(left, right, transposed=False):
    contract = (((1,), (1 if transposed else 0,)), ((), ()))
    plain = left if left.dtype == jnp.bfloat16 else right
    rest = right if left.dtype == jnp.bfloat16 else left
    total = None
    for _ in range(3):
        part = rest.astype(jnp.bfloat16)
        rest = rest - part.astype(jnp.float32)
        pair = (plain, part) if plain is left else (part, plain)
        term = lax.dot_general(*pair, contract, preferred_element_type=jnp.float32)
        total = term if total is None else total + term
    return total


def complex_times(a_real, a_imag, b_real, b_imag):
    return a_real * b_real - a_imag * b_imag, a_real * b_imag + a_imag * b_real


def states_kernel(
    input_hbm,
    shift_hbm,
    pole_real_hbm,
    pole_imag_hbm,
    log_step_hbm,
    map_hbm,
    total_ref,
    drive_real_ref,
    drive_imag_ref,
    scale_ref,
    factor_ref,
    enter_ref,
    input_ref,
    shift_ref,
    pole_real_ref,
    pole_imag_ref,
    log_step_ref,
    map_ref,
    semaphores,
):
    sources = (pole_real_hbm, pole_imag_hbm, log_step_hbm, shift_hbm, input_hbm, map_hbm)
    targets = (pole_real_ref, pole_imag_ref, log_step_ref, shift_ref, input_ref, map_ref)
    copies = [
        pltpu.make_async_copy(source, target, semaphores.at[number])
        for number, (source, target) in enumerate(zip(sources, targets))
    ]
    for copy in copies:
        copy.start()
    for copy in copies:
        copy.wait()
    rows = input_ref.shape[0]
    groups, states = pole_real_ref.shape
    width = groups * states
    channels = map_ref.shape[1] // groups
    length = rows // LANES
    spread = one_hot((states, width), lambda r, c: c % states == r).astype(jnp.bfloat16)
    group_of = one_hot((groups, width), lambda r, c: c // states == r)

    def in_a_row(ref):
        return jnp.sum(whole_dot(ref[...], spread) * group_of, axis=0, keepdims=True)

    pole_real, pole_imag = in_a_row(pole_real_ref), in_a_row(pole_imag_ref)
    logs = jnp.broadcast_to(log_step_ref[...], (groups, groups))
    step = jnp.exp(whole_dot(logs, group_of.astype(jnp.bfloat16))[:1])
    magnitude = jnp.exp(pole_real * step)
    factor_real = magnitude * jnp.cos(pole_imag * step)
    factor_imag = magnitude * jnp.sin(pole_imag * step)
    denominator = pole_real * pole_real + pole_imag * pole_imag
    ratio_real = ((factor_real - 1.0) * pole_real + factor_imag * pole_imag) / denominator
    ratio_imag = (factor_imag * pole_real - (factor_real - 1.0) * pole_imag) / denominator
    factor_ref[0:1, :] = factor_real
    factor_ref[1:2, :] = factor_imag

    order = one_hot((rows, rows), lambda r, c: c == (r % LANES) * length + r // LANES)
    order = order.astype(jnp.bfloat16)
    inputs = jnp.dot(order, input_ref[...], preferred_element_type=jnp.float32)
    inputs = inputs.astype(jnp.bfloat16)
    scale_ref[...] = whole_dot(
        whole_dot(order, jnp.exp(shift_ref[...]), True), group_of.astype(jnp.bfloat16)
    )
    same_group = one_hot(
        (groups * channels, width), lambda r, c: r // channels == c // states
    )
    plain_real = whole_dot(inputs, whole_dot(map_ref[0], spread) * same_group)
    plain_imag = whole_dot(inputs, whole_dot(map_ref[1], spread) * same_group)
    drive_real, drive_imag = complex_times(ratio_real, ratio_imag, plain_real, plain_imag)
    drive_real_ref[...] = drive_real
    drive_imag_ref[...] = drive_imag

    wide_real = jnp.broadcast_to(factor_real, (LANES, width))
    wide_imag = jnp.broadcast_to(factor_imag, (LANES, width))
    through_real = jnp.ones((LANES, width), jnp.float32)
    through_imag = state_real = state_imag = jnp.zeros((LANES, width), jnp.float32)

    def advance(k, held):
        through_real, through_imag, state_real, state_imag = held
        at = pl.ds(pl.multiple_of(k * LANES, LANES), LANES)
        scale = scale_ref[at, :]
        real, imag = scale * wide_real, scale * wide_imag
        through_real, through_imag = complex_times(real, imag, through_real, through_imag)
        state_real, state_imag = complex_times(real, imag, state_real, state_imag)
        state_real = state_real + drive_real_ref[at, :]
        state_imag = state_imag + drive_imag_ref[at, :]
        return through_real, through_imag, state_real, state_imag

    through_real, through_imag, state_real, state_imag = lax.fori_loop(
        0, length, advance, (through_real, through_imag, state_real, state_imag), unroll=4
    )

    place = lax.broadcasted_iota(jnp.int32, (LANES, width), 0)

    def moved(value, by, empty):
        return jnp.where(place >= by, pltpu.roll(value, by, 0), empty)

    by = 1
    while by < LANES:
        a_real, a_imag = moved(through_real, by, 1.0), moved(through_imag, by, 0.0)
        x_real, x_imag = moved(state_real, by, 0.0), moved(state_imag, by, 0.0)
        x_real, x_imag = complex_times(through_real, through_imag, x_real, x_imag)
        state_real, state_imag = state_real + x_real, state_imag + x_imag
        through_real, through_imag = complex_times(through_real, through_imag, a_real, a_imag)
        by *= 2
    enter_ref[0] = moved(through_real, 1, 1.0)
    enter_ref[1] = moved(through_imag, 1, 0.0)
    enter_ref[2] = moved(state_real, 1, 0.0)
    enter_ref[3] = moved(state_imag, 1, 0.0)
    total = jnp.concatenate(
        [v[LANES - 1 :] for v in (through_real, through_imag, state_real, state_imag)], axis=0
    )
    total_ref[...] = jnp.broadcast_to(total[None], total_ref.shape)


def response_kernel(here_ref, *refs):
    sources, (out_ref, state_ref), targets, semaphores = (
        refs[:9],
        refs[9:11],
        refs[11:20],
        refs[20],
    )
    copies = [
        pltpu.make_async_copy(source, target, semaphores.at[number])
        for number, (source, target) in enumerate(zip(sources, targets))
    ]
    for copy in copies:
        copy.start()
    (
        arrived_ref,
        drive_real_ref,
        drive_imag_ref,
        scale_ref,
        factor_ref,
        enter_ref,
        input_ref,
        readout_ref,
        skip_ref,
    ) = targets
    copies[0].wait()
    rows = input_ref.shape[0]
    width = factor_ref.shape[1]
    states = readout_ref.shape[2]
    channels = readout_ref.shape[1] * states // width
    length = rows // LANES
    here = here_ref[0]
    carry_real = carry_imag = jnp.zeros((1, width), jnp.float32)
    for j in range(arrived_ref.shape[0]):
        block = arrived_ref[j]
        real, imag = complex_times(block[0:1], block[1:2], carry_real, carry_imag)
        earlier = j < here
        carry_real = jnp.where(earlier, real + block[2:3], carry_real)
        carry_imag = jnp.where(earlier, imag + block[3:4], carry_imag)
    for copy in copies[1:]:
        copy.wait()
    state_real, state_imag = complex_times(enter_ref[0], enter_ref[1], carry_real, carry_imag)
    state_real, state_imag = state_real + enter_ref[2], state_imag + enter_ref[3]
    wide_real = jnp.broadcast_to(factor_ref[0:1, :], (LANES, width))
    wide_imag = jnp.broadcast_to(factor_ref[1:2, :], (LANES, width))

    def advance(k, held):
        state_real, state_imag = held
        at = pl.ds(pl.multiple_of(k * LANES, LANES), LANES)
        scale = scale_ref[at, :]
        real, imag = scale * wide_real, scale * wide_imag
        state_real, state_imag = complex_times(real, imag, state_real, state_imag)
        state_real = state_real + drive_real_ref[at, :]
        state_imag = state_imag + drive_imag_ref[at, :]
        state_ref[at, :width] = state_real
        state_ref[at, width:] = state_imag
        return state_real, state_imag

    lax.fori_loop(0, length, advance, (state_real, state_imag), unroll=8)
    spread = one_hot((states, width), lambda r, c: c % states == r).astype(jnp.bfloat16)
    same_group = one_hot(
        (readout_ref.shape[1], width), lambda r, c: r // channels == c // states
    )
    matrix = jnp.concatenate(
        [
            whole_dot(readout_ref[0], spread) * same_group,
            whole_dot(readout_ref[1], spread) * -same_group,
        ],
        axis=1,
    )
    response = exact_dot(state_ref[...], matrix, True)
    order = one_hot((rows, rows), lambda r, c: r == (c % LANES) * length + c // LANES)
    response = whole_dot(order.astype(jnp.bfloat16), response) + skip_ref[...] * input_ref[...].astype(jnp.float32)
    out_ref[...] = jax.nn.gelu(response).astype(jnp.bfloat16)


def local_states(
    mixer_input, decay_shift, pole_real, pole_imaginary, log_step, input_map, devices
):
    rows = mixer_input.shape[0]
    groups, states = pole_real.shape
    width = groups * states
    f32 = jnp.float32
    shape = jax.ShapeDtypeStruct
    operands = (
        mixer_input,
        decay_shift.T,
        pole_real,
        pole_imaginary,
        log_step[None],
        jnp.swapaxes(input_map, 2, 3).reshape(2, -1, states),
    )
    return pl.pallas_call(
        states_kernel,
        out_shape=(
            shape((devices, 4, width), f32),
            shape((rows, width), f32),
            shape((rows, width), f32),
            shape((rows, width), f32),
            shape((2, width), f32),
            shape((4, LANES, width), f32),
        ),
        in_specs=[pl.BlockSpec(memory_space=pltpu.HBM)] * len(operands),
        scratch_shapes=[pltpu.VMEM(operand.shape, operand.dtype) for operand in operands]
        + [pltpu.SemaphoreType.DMA((len(operands),))],
        compiler_params=pltpu.CompilerParams(vmem_limit_bytes=60 * 1024 * 1024),
        name="states",
    )(*operands)


def activations(here, arrived, kept, mixer_input, readout_matrix, skip):
    rows, channels = mixer_input.shape
    width = arrived.shape[2]
    operands = (
        arrived,
        *kept,
        mixer_input,
        readout_matrix.reshape(2, channels, -1),
        skip[None],
    )
    return pl.pallas_call(
        response_kernel,
        out_shape=jax.ShapeDtypeStruct((rows, channels), jnp.bfloat16),
        in_specs=[pl.BlockSpec(memory_space=pltpu.SMEM)]
        + [pl.BlockSpec(memory_space=pltpu.HBM)] * len(operands),
        scratch_shapes=[pltpu.VMEM((rows, 2 * width), jnp.float32)]
        + [pltpu.VMEM(operand.shape, operand.dtype) for operand in operands]
        + [pltpu.SemaphoreType.DMA((len(operands),))],
        compiler_params=pltpu.CompilerParams(vmem_limit_bytes=60 * 1024 * 1024),
        name="response",
    )(here.reshape(1), *operands)


def experts_kernel(capacity, count, sets, *refs):
    row_refs, refs = refs[:count], refs[count:]
    weights, outs = refs[: 3 * sets], refs[3 * sets :]
    held, part = row_refs[0].shape[0] // 2, row_refs[0].shape[1]

    def whole_rows(half):
        return one_hot(
            (held, 2 * held),
            lambda r, c: c == r // capacity * (2 * capacity) + r % capacity + half * capacity,
        ).astype(jnp.bfloat16)

    pick = [whole_rows(half) for half in range(2)]
    pieces = [
        jnp.concatenate(
            [jnp.dot(chosen, ref[...], preferred_element_type=jnp.float32) for ref in row_refs],
            axis=0,
        ).astype(jnp.bfloat16)
        for chosen in pick
    ]
    total = None
    for number in range(sets):
        gate_ref, up_ref, down_ref = weights[3 * number : 3 * number + 3]

        def product(ref):
            return sum(
                jnp.dot(
                    piece,
                    ref[half * part : (half + 1) * part, :],
                    preferred_element_type=jnp.float32,
                )
                for half, piece in enumerate(pieces)
            )

        hidden = (jax.nn.silu(product(gate_ref)) * product(up_ref)).astype(jnp.bfloat16)
        out = jnp.dot(hidden, down_ref[...], preferred_element_type=jnp.float32)
        total = out if total is None else total + out
    total = total.astype(jnp.bfloat16)
    for number, ref in enumerate(outs):
        rows = total[number * held : (number + 1) * held]
        ref[...] = sum(
            lax.dot_general(
                pick[half],
                rows[:, half * part : (half + 1) * part],
                (((0,), (0,)), ((), ())),
                preferred_element_type=jnp.float32,
            )
            for half in range(2)
        ).astype(jnp.bfloat16)


def partial_out(rows, weights, capacity):
    count, sets = len(rows), len(weights) // 3
    out = jax.ShapeDtypeStruct(rows[0].shape, jnp.bfloat16)
    flops = count * rows[0].shape[0] * sum(w.size for w in weights)
    return pl.pallas_call(
        functools.partial(experts_kernel, capacity, count, sets),
        out_shape=(out,) * count,
        in_specs=[pl.BlockSpec(memory_space=pltpu.VMEM)] * (count + len(weights)),
        compiler_params=pltpu.CompilerParams(vmem_limit_bytes=12 << 20),
        cost_estimate=pl.CostEstimate(flops=flops, bytes_accessed=0, transcendentals=0),
        name="experts",
    )(*rows, *weights)


def stage_kernel(*refs):
    count = len(refs) // 2
    copies = [
        pltpu.make_async_copy(refs[number], refs[count + number], refs[-1].at[number])
        for number in range(count)
    ]
    for copy in copies:
        copy.start()
    for copy in copies:
        copy.wait()


def staged(arrays):
    return pl.pallas_call(
        stage_kernel,
        out_shape=[jax.ShapeDtypeStruct(array.shape, array.dtype) for array in arrays],
        in_specs=[pl.BlockSpec(memory_space=pltpu.HBM)] * len(arrays),
        out_specs=[pl.BlockSpec(memory_space=pltpu.VMEM)] * len(arrays),
        scratch_shapes=[pltpu.SemaphoreType.DMA((len(arrays),))],
        compiler_params=pltpu.CompilerParams(vmem_limit_bytes=32 << 20),
        cost_estimate=pl.CostEstimate(flops=1 << 33, bytes_accessed=0, transcendentals=0),
        name="stage",
    )(*arrays)


def slot_numbers(route_rows, experts, capacity):
    flat = route_rows.reshape(route_rows.shape[:-2] + (-1,))
    matches = (flat[..., None] == jnp.arange(experts, dtype=jnp.int32)).astype(jnp.int32)
    earlier = jnp.cumsum(matches, axis=-2) - matches
    return flat * capacity + jnp.sum(earlier * matches, axis=-1)


def half_places(slots, capacity):
    first = slots // capacity * (2 * capacity) + slots % capacity
    return jnp.stack([first, first + capacity])


def chip_shift(distance, flip=0):
    size = lax.axis_size("tp")
    chips = size // 2
    return [
        (2 * chip + core, 2 * ((chip + distance) % chips) + (core ^ flip))
        for chip in range(chips)
        for core in range(2)
    ]


def gathered_projection(out_proj):
    chips = lax.axis_size("tp") // 2
    mine = [out_proj] + [
        lax.ppermute(out_proj, "tp", chip_shift(distance)) for distance in range(1, chips)
    ]
    other = [lax.ppermute(block, "tp", chip_shift(0, 1)) for block in mine]
    return (*mine, *other)


def mix_kernel(order_ref, arrived_ref, stream_ref, gain_ref, places_ref, *refs):
    *blocks, mixed_ref, outgoing_ref = refs
    tokens, model = stream_ref.shape
    projected = sum(
        jnp.dot(arrived_ref[order_ref[number]], block[...], preferred_element_type=jnp.float32)
        for number, block in enumerate(blocks)
    )
    mixed = (stream_ref[...].astype(jnp.float32) + projected).astype(jnp.bfloat16)
    mixed_ref[...] = mixed
    wide = mixed.astype(jnp.float32)
    mean = jnp.mean(wide * wide, axis=-1, keepdims=True)
    normed = (wide * lax.rsqrt(mean + EPS) * gain_ref[...]).astype(jnp.bfloat16)
    halves = jnp.concatenate([normed[:, : model // 2], normed[:, model // 2 :]], axis=0)
    width = outgoing_ref.shape[0]
    at = lax.broadcasted_iota(jnp.int32, (2 * tokens, width), 1)
    hits = sum(
        jnp.where(at == places_ref[:, k : k + 1], 1.0, 0.0) for k in range(places_ref.shape[1])
    ).astype(jnp.bfloat16)
    outgoing_ref[...] = lax.dot_general(
        hits, halves, (((0,), (0,)), ((), ())), preferred_element_type=jnp.float32
    ).astype(jnp.bfloat16)


def mixed_and_outgoing(activated, blocks, stream, norm_gain, places, width):
    size = lax.axis_size("tp")
    chips = size // 2
    here = lax.axis_index("tp")
    chip, core = here // 2, here % 2
    tokens, model = stream.shape
    back = 2 * ((chip - jnp.arange(chips, dtype=jnp.int32)) % chips)
    order = jnp.concatenate([back + core, back + 1 - core])
    arrived = lax.all_to_all(
        activated.reshape(size, tokens, -1), "tp", split_axis=0, concat_axis=0, tiled=True
    )
    vmem = pl.BlockSpec(memory_space=pltpu.VMEM)
    shape = jax.ShapeDtypeStruct
    return pl.pallas_call(
        mix_kernel,
        out_shape=(
            shape((tokens, model), jnp.bfloat16),
            shape((width, model // 2), jnp.bfloat16),
        ),
        in_specs=[pl.BlockSpec(memory_space=pltpu.SMEM)]
        + [vmem] * (4 + size),
        compiler_params=pltpu.CompilerParams(vmem_limit_bytes=12 << 20),
        name="mix",
    )(order, arrived, stream, norm_gain[None], places.reshape(2 * tokens, -1), *blocks)


def over_experts(halves, experts):
    blocks = halves.reshape(experts, -1, halves.shape[1])
    return lax.all_to_all(blocks, "sp", split_axis=0, concat_axis=0, tiled=True).reshape(
        halves.shape
    )


def expert_over_chips(rows, w_gate, w_up, w_down, w_up_other, w_down_other, capacity):
    rows, sent, *kept = lax.optimization_barrier(
        (rows, w_gate, w_gate, w_up, w_down, w_up_other, w_down_other)
    )
    before = lax.ppermute(rows, "tp", chip_shift(1))
    after = lax.ppermute(rows, "tp", chip_shift(-1))
    w_gate_other = lax.ppermute(sent, "tp", chip_shift(0, 1))
    w_gate, w_up, w_down, w_up_other, w_down_other = staged(kept)
    weights = (w_gate, w_up, w_down, w_gate_other, w_up_other, w_down_other)
    before, after, *weights = lax.optimization_barrier((before, after, *weights))
    middle = rows.shape[0] // 2
    across = (
        lax.ppermute(before[:middle], "tp", chip_shift(1)),
        lax.ppermute(after[middle:], "tp", chip_shift(-1)),
    )
    (for_before,) = partial_out((before,), weights, capacity)
    to_before = lax.ppermute(for_before, "tp", chip_shift(-1))
    after, for_before = lax.optimization_barrier((after, for_before))
    (for_after,) = partial_out((after,), weights, capacity)
    to_after = lax.ppermute(for_after, "tp", chip_shift(1))
    across, for_after = lax.optimization_barrier((across, for_after))
    for_across = partial_out(across, weights, capacity)
    to_across = [lax.ppermute(part, "tp", chip_shift(2)) for part in for_across]
    rows, _ = lax.optimization_barrier((rows, for_across))
    (total,) = partial_out((rows,), weights, capacity)
    total = total.astype(jnp.float32) + to_before.astype(jnp.float32)
    total = lax.optimization_barrier(total + to_after.astype(jnp.float32))
    total = total + jnp.concatenate(to_across, axis=0).astype(jnp.float32)
    return total.astype(jnp.bfloat16)


def spread_weights(places, weights, width):
    tokens, top = weights.shape
    hits = places.reshape(2, tokens, top)[..., None] == jnp.arange(width, dtype=jnp.int32)
    spread = jnp.sum(jnp.where(hits, weights[None, :, :, None], 0.0), axis=2)
    spread = spread.reshape(2 * tokens, width)
    high = spread.astype(jnp.bfloat16)
    return jnp.concatenate([high, (spread - high.astype(jnp.float32)).astype(jnp.bfloat16)])


def weighted_pick(spread, returned_result):
    parts = jnp.dot(spread, returned_result, preferred_element_type=jnp.float32)
    return parts[: len(parts) // 2] + parts[len(parts) // 2 :]


def shards(
    mixer_input,
    decay_shift,
    pole_real,
    pole_imaginary,
    log_step,
    input_map,
    readout_matrix,
    skip,
    out_proj,
    stream,
    norm_gain,
    routes,
    route_logits,
    w_gate,
    w_up,
    w_down,
):
    w_down_other = lax.ppermute(w_down[0], "tp", chip_shift(0, 1))
    w_up_other = lax.ppermute(w_up[0], "tp", chip_shift(0, 1))
    totals, *kept = local_states(
        mixer_input,
        decay_shift,
        pole_real,
        pole_imaginary,
        log_step,
        input_map,
        lax.axis_size("sp"),
    )
    ends = lax.all_to_all(totals, "sp", split_axis=0, concat_axis=0, tiled=True)
    blocks = gathered_projection(out_proj)
    own_rows, _ = stream.shape
    weights = jax.nn.sigmoid(
        jnp.stack(
            [route_logits[:, 0] - route_logits[:, 1], route_logits[:, 1] - route_logits[:, 0]],
            axis=1,
        )
    )
    experts = lax.axis_size("sp") * w_gate.shape[0]
    capacity = 4 * own_rows // experts
    width = 2 * experts * capacity
    places = half_places(slot_numbers(routes, experts, capacity), capacity)
    spread = spread_weights(places, weights, width)
    ends, spread, places = lax.optimization_barrier((ends, spread, places))
    activated = activations(
        lax.axis_index("sp"), ends, kept, mixer_input, readout_matrix, skip
    )
    mixed, outgoing = mixed_and_outgoing(
        activated, blocks, stream, norm_gain, places, width
    )
    mixed_wide = mixed.astype(jnp.float32)

    arrived = over_experts(outgoing, experts)
    summed = expert_over_chips(
        arrived, w_gate[0], w_up[0], w_down[0], w_up_other, w_down_other, capacity
    )
    picked = weighted_pick(spread, over_experts(summed, experts))
    picked = jnp.concatenate([picked[:own_rows], picked[own_rows:]], axis=1)
    return (mixed_wide + picked).astype(jnp.bfloat16)


def solution(mesh):
    return jax.shard_map(
        shards,
        mesh=mesh,
        in_specs=(
            P("sp", "tp"),
            P("sp", "tp"),
            P("tp", None),
            P("tp", None),
            P("tp"),
            P(None, "tp", None, None),
            P(None, "tp", None, None),
            P("tp"),
            P("tp", None),
            P(("sp", "tp"), None),
            P(),
            P(("sp", "tp"), None),
            P(("sp", "tp"), None),
            P("sp", None, "tp"),
            P("sp", None, "tp"),
            P("sp", "tp", None),
        ),
        out_specs=P(("sp", "tp"), None),
        check_vma=False,
    )
```
